32 devices in a mesh: sp: 8 (over z, y), tp: 4 (over x, core).
Axes of the slice: x: 2, y: 2, z: 4, core: 2. Of those that a mesh axis runs over, the one named last changes fastest.
Arguments:
- out_grad: bfloat16 [1024, 2048], P('sp', 'tp'), may hold values from -6 to 6
- route_ids: int32 [1024, 2], P('sp'), may hold values from 0 to 7, as said below
- route_weight: float32 [1024, 2], P('sp'), may hold values from 0.1 to 0.9
- expert_inputs: bfloat16 [8, 512, 2048], P('sp'), may hold values from -6 to 6
- gate_weight: bfloat16 [8, 2048, 3072], P('sp', None, 'tp'), may hold values from -0.125 to 0.125
- up_weight: bfloat16 [8, 2048, 3072], P('sp', None, 'tp'), may hold values from -0.125 to 0.125
- down_weight: bfloat16 [8, 3072, 2048], P('sp', 'tp'), may hold values from -0.109375 to 0.109375
- out_gate: bfloat16 [1024, 2048], P('sp', 'tp'), may hold values from -6 to 6
- in_gate: bfloat16 [1024, 2048], P('sp', 'tp'), may hold values from -6 to 6
- values: bfloat16 [1024, 2048], P('sp', 'tp'), may hold values from -6 to 6
- conv_out: bfloat16 [1024, 2048], P('sp', 'tp'), may hold values from -6 to 6
- conv_taps: bfloat16 [3, 2048], P(None, 'tp'), may hold values from -3.5 to 3.5
- proj_weight: bfloat16 [2048, 2048], P(None, 'tp'), may hold values from -0.125 to 0.125
Outputs:
- resid_grad: bfloat16 [1024, 2048], P('sp', 'tp')
- out_gate_grad: bfloat16 [1024, 2048], P('sp', 'tp')
- in_gate_grad: bfloat16 [1024, 2048], P('sp', 'tp')
- values_grad: bfloat16 [1024, 2048], P('sp', 'tp')
- proj_grad: float32 [2048, 2048], P('sp', 'tp')
- gate_grad: bfloat16 [8, 2048, 3072], P('sp', None, 'tp')
- up_grad: bfloat16 [8, 2048, 3072], P('sp', None, 'tp')
- down_grad: bfloat16 [8, 3072, 2048], P('sp', 'tp')
The draws below stay inside these ranges and needn't reach their ends.
Inputs may be any that keep to these rules, and one draw needn't show every extreme that they name: `route_ids`: each row names two different experts. Among the rows of one device (aligned blocks of 128 rows) no expert is named more than 64 times, and in every draw one expert is named exactly 64 times in every block.
All inputs are finite; a program needn't handle non-finite values.
Results may differ from the reference program's by a relative error of at most 0.017.
Values may be sent and summed in bfloat16 or wider, within the bound.
A program may use at most 128 MiB of HBM per device.

```python
import math
import jax
import jax.numpy as jnp
from jax import lax

D = 2048
FF = 3072
TAPS = 3
TOK_DEV = 128
TOKENS = 1024
EXPERTS = 8
CAP = 64
SLOTS = 512
N_TP = 4


def draw_route_ids(key, part):
    blocks = TOKENS // TOK_DEV
    tickets = jnp.arange(EXPERTS * CAP, dtype=jnp.int32) // CAP
    filled = jax.random.randint(jax.random.fold_in(key, 11), (), 0, EXPERTS)

    def one_block(block_key):
        extra = jax.random.randint(jax.random.fold_in(block_key, 1), (), 0, EXPERTS)
        shuffled = tickets[jax.random.permutation(jax.random.fold_in(block_key, 2), EXPERTS * CAP)]
        priority = jnp.where(shuffled == filled, 0, jnp.where(shuffled == extra, 1, 2)).astype(jnp.int32)
        chosen = shuffled[jnp.argsort(priority, stable=True)][:2 * TOK_DEV]
        ordered = jnp.sort(chosen)
        pairs = jnp.stack([ordered[:TOK_DEV], ordered[TOK_DEV:]], axis=1)
        flips = jax.random.randint(jax.random.fold_in(block_key, 3), (TOK_DEV, 1), 0, 2)
        pairs = jnp.where(flips == 1, pairs[:, ::-1], pairs)
        shuffle_rows = jax.random.permutation(jax.random.fold_in(block_key, 4), TOK_DEV)
        return pairs[shuffle_rows]
    block_keys = jax.random.split(jax.random.fold_in(key, 7), blocks)
    return jax.vmap(one_block)(block_keys).reshape(TOKENS, 2).astype(jnp.int32)


def spiked(values, key, source, target, blocks, factor):
    def block_of(position):
        return (jnp.arange(values.shape[position]) // (values.shape[position] // blocks)).reshape((-1,) + (1,) * (values.ndim - 1 - position))

    first = jax.random.permutation(key, blocks)[block_of(target)]
    other_side = (block_of(target) + blocks // 2) % blocks
    return jnp.where((block_of(source) == first) | (block_of(source) == other_side), factor * values, values)


def levels(rng, extent, pieces, least, largest):
    level, own = 1.0, jax.random.fold_in(rng, 6)
    for axis_at, parts in pieces:
        heights = jnp.exp(jax.random.uniform(jax.random.fold_in(own, axis_at), (parts,), jnp.float32, least / len(pieces), largest / len(pieces)))
        level = level * jnp.repeat(heights, extent[axis_at] // parts).reshape([-1 if axis == axis_at else 1 for axis in range(len(extent))])
    return level


def centred(own_key, dims, deviation, reach, cuts=(), held_as=jnp.bfloat16):
    level = levels(own_key, dims, cuts, -0.22, 0.18) if cuts else 1.0
    entries = jax.random.normal(own_key, dims, jnp.float32) * deviation * level
    return jnp.minimum(jnp.maximum(entries, -reach), reach).astype(held_as)


def bell_draw_with(own_key, shape, scale, bound, shards, heavy, kind=jnp.bfloat16):
    values = scale * jax.random.normal(own_key, shape, jnp.float32)
    if shards:
        values = values * levels(own_key, shape, shards, -0.22, 0.18)
    return jnp.clip(spiked(values, jax.random.fold_in(own_key, 3), *heavy), -bound, bound).astype(kind)


def setup_inputs(seed: int = 0) -> dict:
    streams_of = jax.random.split(jax.random.key(seed), 14)
    out_grad = bell_draw_with(streams_of[0], (TOKENS, D), 1.0, 6.0, ((0, 8), (1, 4)), (0, 1, 8, 2.0))
    route_ids = draw_route_ids(jax.random.fold_in(streams_of[13], 71), 0)
    route_weight = jnp.clip(0.1 + 0.79999997 * jax.random.uniform(streams_of[2], (TOKENS, 2), jnp.float32) ** levels(streams_of[2], (TOKENS, 2), ((0, 8),), -0.2, 0.2), 0.1, 0.9)
    expert_inputs = centred(streams_of[3], (EXPERTS, SLOTS, D), 1.0, 6.0, ((0, 8),))
    gate_weight = centred(streams_of[4], (EXPERTS, D, FF), D ** -0.5, 0.125, ((0, 8), (2, 4)))
    up_weight = centred(streams_of[5], (EXPERTS, D, FF), D ** -0.5, 0.125, ((0, 8), (2, 4)))
    down_weight = centred(streams_of[6], (EXPERTS, FF, D), FF ** -0.5, 0.109375, ((0, 8), (1, 4)))
    out_gate = centred(streams_of[7], (TOKENS, D), 1.0, 6.0, ((0, 8), (1, 4)))
    in_gate = centred(streams_of[8], (TOKENS, D), 1.0, 6.0, ((0, 8), (1, 4)))
    values = centred(streams_of[9], (TOKENS, D), 1.0, 6.0, ((0, 8), (1, 4)))
    conv_out = centred(streams_of[10], (TOKENS, D), 1.0, 6.0, ((0, 8), (1, 4)))
    conv_taps = centred(streams_of[11], (TAPS, D), TAPS ** -0.5, 3.5, ((1, 4),))
    proj_weight = centred(streams_of[12], (D, D), D ** -0.5, 0.125, ((1, 4),))
    return dict(out_grad=out_grad, route_ids=route_ids, route_weight=route_weight, expert_inputs=expert_inputs, gate_weight=gate_weight, up_weight=up_weight, down_weight=down_weight, out_gate=out_gate, in_gate=in_gate, values=values, conv_out=conv_out, conv_taps=conv_taps, proj_weight=proj_weight)


def slot_rows(route_ids):
    blocks = route_ids.reshape(TOKENS // TOK_DEV, 2 * TOK_DEV)
    onehot = (blocks[:, :, None] == jnp.arange(EXPERTS, dtype=jnp.int32)[None, None, :]).astype(jnp.int32)
    ranked = lax.optimization_barrier(jnp.sum((jnp.cumsum(onehot, axis=1) - onehot) * onehot, axis=2))
    source = jnp.arange(TOKENS // TOK_DEV, dtype=jnp.int32)[:, None]
    return (blocks * SLOTS + source * CAP + ranked).reshape(-1).astype(jnp.int32)

def expert_step(operands):
    inputs, routed, gate_w, up_w, down_w = operands
    pre_gate = jnp.dot(inputs, gate_w, preferred_element_type=jnp.float32)
    pre_up = jnp.dot(inputs, up_w, preferred_element_type=jnp.float32)
    sigmoid_g = jax.nn.sigmoid(pre_gate)
    activated = pre_gate * sigmoid_g
    hidden = (activated * pre_up).astype(jnp.bfloat16)
    d_hidden = jnp.dot(routed, down_w.T, preferred_element_type=jnp.float32)
    d_gate = (d_hidden * pre_up * sigmoid_g * (1.0 + pre_gate * (1.0 - sigmoid_g))).astype(jnp.bfloat16)
    d_up = (d_hidden * activated).astype(jnp.bfloat16)
    slot_scale = 1.0 / math.sqrt(SLOTS)
    gate_grad = (jnp.dot(inputs.T, d_gate, preferred_element_type=jnp.float32) * slot_scale).astype(jnp.bfloat16)
    up_grad = (jnp.dot(inputs.T, d_up, preferred_element_type=jnp.float32) * slot_scale).astype(jnp.bfloat16)
    down_grad = (jnp.dot(hidden.T, routed, preferred_element_type=jnp.float32) * slot_scale).astype(jnp.bfloat16)
    block_width = FF // N_TP
    back = jnp.zeros((SLOTS, D), jnp.float32)
    for block in range(N_TP):
        lower = block * block_width
        upper = lower + block_width
        part_sum = jnp.dot(lax.slice_in_dim(d_gate, lower, upper, axis=1), lax.slice_in_dim(gate_w, lower, upper, axis=1).T, preferred_element_type=jnp.float32)
        part_sum = part_sum + jnp.dot(lax.slice_in_dim(d_up, lower, upper, axis=1), lax.slice_in_dim(up_w, lower, upper, axis=1).T, preferred_element_type=jnp.float32)
        back = back + lax.optimization_barrier(part_sum.astype(jnp.bfloat16)).astype(jnp.float32)
    return (gate_grad, up_grad, down_grad, back.astype(jnp.bfloat16))

def reference(out_grad, route_ids, route_weight, expert_inputs, gate_weight, up_weight, down_weight, out_gate, in_gate, values, conv_out, conv_taps, proj_weight):
    rows = slot_rows(route_ids)
    weighted = (route_weight[:, :, None] * out_grad.astype(jnp.float32)[:, None, :]).astype(jnp.bfloat16).reshape(2 * TOKENS, D)
    routed = jnp.zeros((EXPERTS * SLOTS, D), jnp.bfloat16).at[rows].set(weighted).reshape(EXPERTS, SLOTS, D)
    gate_grad, up_grad, down_grad, back = lax.map(expert_step, (expert_inputs, routed, gate_weight, up_weight, down_weight))
    pair_back = back.reshape(EXPERTS * SLOTS, D)[rows].astype(jnp.float32).reshape(TOKENS, 2, D)
    resid_grad = (out_grad.astype(jnp.float32) + pair_back[:, 0] + pair_back[:, 1]).astype(jnp.bfloat16)
    gate_vals = out_gate.astype(jnp.float32)
    conv_vals = conv_out.astype(jnp.float32)
    mixed_in = (gate_vals * conv_vals).astype(jnp.bfloat16)
    proj_grad = jnp.dot(resid_grad.T, mixed_in, preferred_element_type=jnp.float32) * (1.0 / math.sqrt(TOKENS))
    mix_grad = jnp.dot(resid_grad, proj_weight, preferred_element_type=jnp.float32)
    out_gate_grad = (mix_grad * conv_vals).astype(jnp.bfloat16)
    conv_grad = lax.optimization_barrier((mix_grad * gate_vals).astype(jnp.bfloat16)).astype(jnp.float32)
    padded = jnp.pad(conv_grad, ((1, 1), (0, 0)))
    tap_vals = conv_taps.astype(jnp.float32)
    value_grad = padded[2:] * tap_vals[0] + padded[1:-1] * tap_vals[1] + padded[:-2] * tap_vals[2]
    in_gate_grad = (value_grad * values.astype(jnp.float32)).astype(jnp.bfloat16)
    values_grad = (value_grad * in_gate.astype(jnp.float32)).astype(jnp.bfloat16)
    return (resid_grad, out_gate_grad, in_gate_grad, values_grad, proj_grad, gate_grad, up_grad, down_grad)
```

```python
import functools
import math

import jax
import jax.numpy as jnp
from jax import lax
from jax.experimental import pallas as pl
from jax.experimental.pallas import tpu as pltpu
from jax.sharding import PartitionSpec as P

BF = jnp.bfloat16
F32 = jnp.float32
MESH = pl.DeviceIdType.MESH
VMEM = pl.BlockSpec(memory_space=pltpu.VMEM)
HBM = pl.BlockSpec(memory_space=pltpu.HBM)
NT = ((1,), (1,))
NN = ((1,), (0,))


def dot(left, right, dims):
    return lax.dot_general(left, right, (dims, ((), ())), preferred_element_type=F32)


def remote(src, dst, send, recv, device):
    return pltpu.make_async_remote_copy(
        src_ref=src, dst_ref=dst, send_sem=send, recv_sem=recv, device_id=device, device_id_type=MESH
    )


def span(index, size):
    return pl.ds(pl.multiple_of(index * size, size), size)


def flip(s, m, n):
    out, bit = 0, 1
    while bit < n:
        out = out + bit * lax.rem(lax.div(s, bit) + (m // bit if isinstance(m, int) else lax.div(m, bit)), 2)
        bit *= 2
    return out


def low(m):
    return m & -m


def layer_kernel(
    n_sp, n_tp, experts, slot_scale,
    grad_hbm, ids_hbm, rw_hbm, x_hbm, gw_hbm, uw_hbm, dw_hbm,
    og_hbm, ig_hbm, val_hbm, conv_hbm, taps_hbm, pw_hbm,
    resid, og_out, ig_out, val_out, columns, zall, ggrad, ugrad, dgrad,
    grad, ids, rw, x, w, dw, og, ig, val, conv, taps, pw,
    xt, pre, routed, hidden, dall, outgoing, parts, from_sib, far_out, far_in, total, final, back, disp,
    rfull, pieces, edge_out, edge_in,
    load_sems, ex_sems, sib_sems, far_sems, ret_sems, gat_sems, z_sems, e_sems, halo_sems,
):
    me, tp = lax.axis_index("sp"), lax.axis_index("tp")
    core = lax.rem(tp, 2)
    sib = tp + 1 - 2 * core
    far = lax.rem(tp + n_tp // 2, n_tp)
    far_sib = lax.rem(sib + n_tp // 2, n_tp)
    tokens, chan = grad.shape
    slots, width = x.shape
    hid = dw.shape[0]
    cap = slots // n_sp
    half, quarter = n_sp // 2, n_sp // 4
    piece = width // n_sp
    per_block = chan // piece
    share = tokens // 2
    tile = 256

    pairs = [
        (grad_hbm, grad), (ids_hbm, ids), (rw_hbm, rw), (og_hbm, og), (conv_hbm, conv),
        (x_hbm.at[0], x), (gw_hbm.at[0], w.at[:, pl.ds(0, hid)]), (uw_hbm.at[0], w.at[:, pl.ds(hid, hid)]),
        (dw_hbm.at[0], dw), (ig_hbm, ig), (val_hbm, val), (taps_hbm, taps), (pw_hbm, pw),
    ]
    loads = [pltpu.make_async_copy(a, b, load_sems.at[i]) for i, (a, b) in enumerate(pairs)]
    for load in loads[:3]:
        load.start()
    barrier = pltpu.get_barrier_semaphore()
    for m in range(1, n_sp):
        pl.semaphore_signal(barrier, inc=1, device_id={"sp": flip(me, m, n_sp)}, device_id_type=MESH)
    for other in (sib, far):
        pl.semaphore_signal(barrier, inc=1, device_id={"tp": other}, device_id_type=MESH)
    for load in loads[3:]:
        load.start()
    for load in loads[:3]:
        load.wait()

    id0, id1 = ids[0:1, :], ids[1:2, :]
    names = lax.broadcasted_iota(jnp.int32, (experts, tokens), 0)
    hit0 = jnp.where(id0 == names, 1.0, 0.0).astype(F32)
    hit1 = jnp.where(id1 == names, 1.0, 0.0).astype(F32)
    rows = lax.broadcasted_iota(jnp.int32, (tokens, tokens), 0)
    cols = lax.broadcasted_iota(jnp.int32, (tokens, tokens), 1)
    earlier = jnp.where(rows < cols, 1.0, 0.0).astype(BF)
    counts = dot((hit0 + hit1).astype(BF), earlier, NN)
    slot0 = id0.astype(F32) * float(cap) + jnp.sum(counts * hit0, axis=0, keepdims=True)
    slot1 = id1.astype(F32) * float(cap) + jnp.sum(counts * hit1, axis=0, keepdims=True)
    places = lax.broadcasted_iota(jnp.int32, (experts * cap, tokens), 0).astype(F32)
    at0, at1 = slot0 == places, slot1 == places
    weight = jnp.sum(
        jnp.where(at0, rw[0:1, :], 0.0) + jnp.where(at1, rw[1:2, :], 0.0), axis=1, keepdims=True
    )
    chosen = (jnp.where(at0, 1.0, 0.0) + jnp.where(at1, 1.0, 0.0)).astype(BF)
    outgoing[...] = (dot(chosen, grad[...], NN) * weight).astype(BF)

    pl.semaphore_wait(barrier, n_sp + 1)

    def row_at(s):
        return span(s, cap)

    def place(j, s):
        return routed.at[row_at(s), span(j, chan)]

    def sp_copy(m):
        to = flip(me, m, n_sp)
        return remote(
            outgoing.at[row_at(to), :], place(tp, me), ex_sems.at[0, m], ex_sems.at[1, m], {"sp": to}
        )

    def far_share(m):
        at = place(tp, flip(me, m, n_sp))
        return remote(at, at, ex_sems.at[2, m], ex_sems.at[3, m], {"tp": far})

    def sib_share(m):
        at = place(tp, flip(me, m, n_sp))
        return remote(at, at, ex_sems.at[4, m], ex_sems.at[5, m], {"tp": sib})

    def hand_share(m):
        at = place(far, flip(me, m, n_sp))
        return remote(at, at, ex_sems.at[6, m], ex_sems.at[7, m], {"tp": sib})

    def spread(m):
        sp_copy(m).wait_recv()
        far_share(m).start()
        sib_share(m).start()

    def hand(m):
        far_share(m).wait_recv()
        hand_share(m).start()

    @pl.loop(1, n_sp)
    def _(m):
        sp_copy(m).start()

    own = pltpu.make_async_copy(outgoing.at[row_at(me), :], place(tp, me), ex_sems.at[0, 0])
    own.start()
    own.wait()
    far_share(0).start()
    sib_share(0).start()

    loads[3].wait()
    loads[4].wait()
    zall[me] = (og[...].astype(F32) * conv[...].astype(F32)).astype(BF)
    disp[...] = chosen.T

    def z_copy(result, bit):
        block = flip(me, result - bit, n_sp)
        return remote(
            zall.at[block], zall.at[block], z_sems.at[0, result], z_sems.at[1, result],
            {"sp": flip(me, bit, n_sp)},
        )

    def z_send(m):
        bit = low(m) // 2 if m else half // 2
        while bit:
            z_copy(m + bit, bit).start()
            bit //= 2

    def z_forward(m):
        if low(m) > 1:
            z_copy(m, low(m)).wait_recv()
            z_send(m)

    z_send(0)

    def pre_dot(t):
        at = span(t, tile)
        pre[:, at] = dot(x[...], w[:, at], NN)

    for load in loads[5:8]:
        load.wait()
    pre_tiles = 2 * hid // tile
    first = min(pre_tiles, half)
    spread(1)

    @pl.loop(0, first)
    def _(t):
        spread(t + 2)
        pre_dot(t)
        hand(t)

    if first < pre_tiles:
        pl.loop(first, pre_tiles)(pre_dot)

    if first < half:
        @pl.loop(first, half)
        def _(t):
            spread(t + 2)
            hand(t)

    @pl.loop(0, half)
    def _(m):
        sib_share(m).wait_recv()
        hand_share(m).wait_recv()

    loads[8].wait()

    def hidden_rows(at, t):
        cols_at, up_at = span(t, tile), pl.ds(pl.multiple_of(hid + t * tile, tile), tile)
        d_hidden = dot(routed[at, :], dw[cols_at, :], NT)
        gate, up = pre[at, cols_at], pre[at, up_at]
        sig = jax.nn.sigmoid(gate)
        act = gate * sig
        hidden[at, cols_at] = (act * up).astype(BF)
        dall[at, cols_at] = (d_hidden * up * sig * (1.0 + gate * (1.0 - sig))).astype(BF)
        dall[at, up_at] = (d_hidden * act).astype(BF)

    def hidden_group(at):
        pl.loop(0, hid // tile)(lambda t: hidden_rows(at, t))

    near = span(lax.div(me, half), half * cap)
    fars = [span(flip(lax.div(me, quarter), 2 + i, 4), quarter * cap) for i in range(2)]
    group = [*fars, near]
    hidden_group(near)

    @pl.loop(0, width // tile)
    def _(t):
        at = span(t, tile)
        xt[at, :] = x[:, at].T

    @pl.loop(half, half + quarter)
    def _(m):
        spread(m + 2)
        hand(m)

    z_copy(half, half).start()

    def back_part(at, block, out):
        @pl.loop(0, chan // tile)
        def _(t):
            cols_at = span(t, tile)
            value = dot(dall[at, :], w[span(block * (chan // tile) + t, tile), :], NT)
            parts[out, at, cols_at] = value.astype(BF)

    def sib_copy(g, i):
        return remote(
            parts.at[2 * i, group[g], :], from_sib.at[i, group[g], :],
            sib_sems.at[0, 2 * g + i], sib_sems.at[1, 2 * g + i], {"tp": sib},
        )

    def far_copy(m):
        at = row_at(flip(me, m, n_sp))
        return remote(far_out.at[at, :], far_in.at[at, :], far_sems.at[0, m], far_sems.at[1, m], {"tp": far})

    def ret_copy(m):
        to = flip(me, m, n_sp)
        return remote(
            final.at[row_at(to), :], back.at[row_at(me), :], ret_sems.at[0, m], ret_sems.at[1, m], {"sp": to}
        )

    def far_half(g, masks, between):
        at = group[g]
        back_part(at, far_sib, 0)
        sib_copy(g, 0).start()
        back_part(at, far, 1)
        between()
        sib_copy(g, 0).wait_recv()

        @pl.loop(*masks)
        def _(m):
            m = lax.rem(m, n_sp)
            r = row_at(flip(me, m, n_sp))
            far_out[r, :] = (parts[1, r, :].astype(F32) + from_sib[0, r, :].astype(F32)).astype(BF)
            far_copy(m).start()

    def near_half(g):
        at = group[g]
        back_part(at, sib, 2)
        sib_copy(g, 1).start()
        back_part(at, tp, 3)

    def finish_half(g):
        at = group[g]
        sib_copy(g, 1).wait_recv()
        total[at, :] = parts[3, at, :].astype(F32) + from_sib[1, at, :].astype(F32)

    def give(m):
        r = row_at(flip(me, m, n_sp))
        far_copy(m).wait_recv()
        final[r, :] = (total[r, :] + far_in[r, :].astype(F32)).astype(BF)
        ret_copy(m).start()

    def arrived(lo, hi):
        @pl.loop(lo, hi)
        def _(m):
            sib_share(m).wait_recv()
            hand_share(m).wait_recv()

    last = half + quarter
    arrived(half, last)
    hidden_group(fars[0])

    def hand_early():
        @pl.loop(last, n_sp)
        def _(m):
            if last + 2 < n_sp:
                pl.when(m + 2 < n_sp)(lambda: spread(m + 2))
            hand(m)

    far_half(0, (half, last), lambda: None)
    hand_early()
    near_half(0)
    arrived(last, n_sp)
    hidden_group(fars[1])
    far_half(1, (last, n_sp), lambda: None)
    for m in range(1, half):
        z_forward(m)
    finish_half(0)
    far_half(2, (1, half + 1) if half == n_sp else (1, half), lambda: None)
    r0 = row_at(me)
    far_out[r0, :] = (parts[1, r0, :].astype(F32) + from_sib[0, r0, :].astype(F32)).astype(BF)
    far_copy(0).start()
    pl.loop(half, last)(give)
    near_half(1)
    finish_half(1)
    pl.loop(last, n_sp)(give)
    near_half(2)
    finish_half(2)
    for m in range(half, n_sp):
        z_forward(m) if m == half else None

    chunks = width // tile
    each = -(-chunks // half)

    def in_chunk(i):
        at = span(i, tile)
        left = xt[at, :]
        ggrad[0, at, :] = (dot(left, dall[:, :hid], NN) * slot_scale).astype(BF)
        ugrad[0, at, :] = (dot(left, dall[:, hid:], NN) * slot_scale).astype(BF)

    def fill(i):
        for j in range(each):
            c = i * each + j
            if each * half > chunks:
                pl.when(c < chunks)(functools.partial(in_chunk, c))
            else:
                in_chunk(c)

    @pl.loop(1, half)
    def _(m):
        fill(m - 1)
        give(m)

    fill(half - 1)
    for m in range(half + 1, n_sp):
        z_forward(m)
    far_copy(0).wait_recv()
    back[r0, :] = (total[r0, :] + far_in[r0, :].astype(F32)).astype(BF)

    @pl.loop(0, hid // tile)
    def _(t):
        at = span(t, tile)
        dgrad[0, at, :] = (dot(hidden[:, at].T, routed[...], NN) * slot_scale).astype(BF)

    for load in loads[9:]:
        load.wait()

    @pl.loop(1, n_sp)
    def _(m):
        ret_copy(m).wait_recv()

    value = (grad[...].astype(F32) + dot(disp[...], back[...], NN)).astype(BF)
    resid[...] = value
    rfull[tp] = value
    close = remote(rfull.at[tp], rfull.at[tp], gat_sems.at[0], gat_sems.at[1], {"tp": sib})
    away = remote(rfull.at[tp], rfull.at[tp], gat_sems.at[2], gat_sems.at[3], {"tp": far})
    away.start()
    close.start()

    def e_copy(k, m):
        return remote(
            pieces.at[k, core], columns.at[me, core], e_sems.at[0, m], e_sems.at[1, m], {"sp": k}
        )

    def send_pieces(block):
        for j in range(per_block):
            k = block * per_block + j
            at = pl.ds(j * piece, piece)
            for c in range(2):
                pieces[k, c] = rfull[block, pl.ds(c * share, share), at]

            @pl.when(k != me)
            def _():
                e_copy(k, flip(me, k, n_sp)).start()

            @pl.when(k == me)
            def _():
                for c in range(2):
                    columns[me, c] = rfull[block, pl.ds(c * share, share), at]

    def mix_part(block):
        return dot(rfull[block], pw[span(block, chan), :], NN)

    send_pieces(tp)
    mix = mix_part(tp)
    close.wait_recv()
    send_pieces(sib)
    mix = mix + mix_part(sib)
    away.wait_recv()
    passed = remote(rfull.at[far], rfull.at[far], gat_sems.at[4], gat_sems.at[5], {"tp": sib})
    passed.start()
    send_pieces(far)
    mix = mix + mix_part(far)
    passed.wait_recv()
    send_pieces(far_sib)
    mix = mix + mix_part(far_sib)

    conv_grad = (mix * og[...].astype(F32)).astype(BF).astype(F32)
    edge_out[0] = jnp.broadcast_to(conv_grad[tokens - 1:tokens, :], edge_out.shape[1:])
    edge_out[1] = jnp.broadcast_to(conv_grad[0:1, :], edge_out.shape[1:])
    sides = [lax.rem(me + 1, n_sp), lax.rem(me + n_sp - 1, n_sp)]
    halos = [
        remote(edge_out.at[i], edge_in.at[i], halo_sems.at[0, i], halo_sems.at[1, i], {"sp": sides[i]})
        for i in range(2)
    ]
    for halo in halos:
        halo.start()
    og_out[...] = (mix * conv[...].astype(F32)).astype(BF)

    def e_share(m):
        at = columns.at[flip(me, m, n_sp), core]
        return remote(at, at, e_sems.at[2, m], e_sems.at[3, m], {"tp": sib})

    @pl.loop(1, n_sp)
    def _(m):
        e_copy(flip(me, m, n_sp), m).wait_recv()
        e_share(m).start()

    for halo in halos:
        halo.wait()
    before = jnp.where(me == 0, 0.0, edge_in[0, 0:1, :])
    after = jnp.where(me == n_sp - 1, 0.0, edge_in[1, 0:1, :])
    row = lax.broadcasted_iota(jnp.int32, (tokens, chan), 0)
    prev = jnp.where(row == 0, before, pltpu.roll(conv_grad, 1, 0))
    following = jnp.where(row == tokens - 1, after, pltpu.roll(conv_grad, tokens - 1, 0))
    tap = taps[...].astype(F32)
    value_grad = following * tap[0:1, :] + conv_grad * tap[1:2, :] + prev * tap[2:3, :]
    ig_out[...] = (value_grad * val[...].astype(F32)).astype(BF)
    val_out[...] = (value_grad * ig[...].astype(F32)).astype(BF)

    @pl.loop(0, n_sp)
    def _(m):
        far_share(m).wait_send()
        sib_share(m).wait_send()
        hand_share(m).wait_send()
        far_copy(m).wait_send()

    @pl.loop(1, n_sp)
    def _(m):
        sp_copy(m).wait_send()
        ret_copy(m).wait_send()
        e_copy(flip(me, m, n_sp), m).wait_send()
        e_share(m).wait_send()
        e_share(m).wait_recv()

    for g in range(3):
        for i in range(2):
            sib_copy(g, i).wait_send()
    for m in range(1, n_sp):
        z_copy(m, low(m)).wait_send()
        if low(m) == 1:
            z_copy(m, 1).wait_recv()
    for copy in (close, away, passed):
        copy.wait_send()


def finish_kernel(scale, columns, zall, *refs):
    grads, outs, proj, stage, sems = refs[:7], refs[7:14], refs[14], refs[15], refs[16]
    copies = [pltpu.make_async_copy(a, b, sems.at[i]) for i, (a, b) in enumerate(zip(grads, outs))]
    for copy in copies:
        copy.start()
    n_sp, parts, share, piece = columns.shape
    tokens = n_sp * parts * share
    left = columns[...].reshape(tokens, piece).T
    stage[...] = dot(left, zall[...].reshape(tokens, zall.shape[2]), NN) * scale
    last = pltpu.make_async_copy(stage, proj, sems.at[7])
    last.start()
    for copy in copies:
        copy.wait()
    last.wait()


def per_device(
    out_grad, route_ids, route_weight, expert_inputs, gate_weight, up_weight, down_weight,
    out_gate, in_gate, values, conv_out, conv_taps, proj_weight,
):
    n_sp, n_tp = lax.axis_size("sp"), lax.axis_size("tp")
    tokens, chan = out_grad.shape
    local, slots, width = expert_inputs.shape
    hid = gate_weight.shape[2]
    assert local == 1 and n_tp == 4 and n_sp & (n_sp - 1) == 0
    piece = width // n_sp
    dma = pltpu.SemaphoreType.DMA
    rows = jax.ShapeDtypeStruct((tokens, chan), BF)
    wide = jax.ShapeDtypeStruct((1, width, hid), BF)
    tall = jax.ShapeDtypeStruct((1, hid, width), BF)
    small = pltpu.VMEM((tokens, chan), BF)
    slab = pltpu.VMEM((slots, chan), BF)

    resid, og_out, ig_out, val_out, columns, zall, ggrad, ugrad, dgrad = pl.pallas_call(
        functools.partial(layer_kernel, n_sp, n_tp, n_sp * local, 1.0 / math.sqrt(slots)),
        out_shape=[
            rows, rows, rows, rows,
            jax.ShapeDtypeStruct((n_sp, 2, tokens // 2, piece), BF),
            jax.ShapeDtypeStruct((n_sp, tokens, chan), BF),
            wide, wide, tall,
        ],
        in_specs=[HBM] * 13,
        out_specs=[VMEM] * 9,
        scratch_shapes=[
            small,
            pltpu.VMEM((2, tokens), jnp.int32),
            pltpu.VMEM((2, tokens), F32),
            pltpu.VMEM((slots, width), BF),
            pltpu.VMEM((width, 2 * hid), BF),
            pltpu.VMEM((hid, width), BF),
            small, small, small, small,
            pltpu.VMEM(conv_taps.shape, BF),
            pltpu.VMEM(proj_weight.shape, BF),
            pltpu.VMEM((width, slots), BF),
            pltpu.VMEM((slots, 2 * hid), F32),
            pltpu.VMEM((slots, width), BF),
            pltpu.VMEM((slots, hid), BF),
            pltpu.VMEM((slots, 2 * hid), BF),
            slab,
            pltpu.VMEM((4, slots, chan), BF),
            pltpu.VMEM((2, slots, chan), BF),
            slab, slab,
            pltpu.VMEM((slots, chan), F32),
            slab, slab,
            pltpu.VMEM((tokens, slots), BF),
            pltpu.VMEM((n_tp, tokens, chan), BF),
            pltpu.VMEM((n_sp, 2, tokens // 2, piece), BF),
            pltpu.VMEM((2, 8, chan), F32),
            pltpu.VMEM((2, 8, chan), F32),
            dma((13,)), dma((8, n_sp)), dma((2, 6)), dma((2, n_sp)), dma((2, n_sp)), dma((6,)),
            dma((2, n_sp)), dma((4, n_sp)), dma((2, 2)),
        ],
        compiler_params=pltpu.CompilerParams(
            collective_id=0, has_side_effects=True, vmem_limit_bytes=44 * 2**20
        ),
        name="layer",
    )(*(
        pltpu.with_memory_space_constraint(a, pltpu.HBM) for a in (
            out_grad, route_ids.T, route_weight.T, expert_inputs, gate_weight, up_weight, down_weight,
            out_gate, in_gate, values, conv_out, conv_taps, proj_weight,
        )
    ))
    resid, og_out, ig_out, val_out, ggrad, ugrad, dgrad, proj_grad = pl.pallas_call(
        functools.partial(finish_kernel, 1.0 / math.sqrt(tokens * n_sp)),
        out_shape=[rows, rows, rows, rows, wide, wide, tall, jax.ShapeDtypeStruct((piece, chan), F32)],
        in_specs=[VMEM] * 9,
        out_specs=[HBM] * 8,
        scratch_shapes=[pltpu.VMEM((piece, chan), F32), dma((8,))],
        compiler_params=pltpu.CompilerParams(vmem_limit_bytes=6 * 2**20),
        name="finish",
    )(columns, zall, resid, og_out, ig_out, val_out, ggrad, ugrad, dgrad)
    return resid, og_out, ig_out, val_out, proj_grad, ggrad, ugrad, dgrad


def solution(mesh):
    rows = P("sp", "tp")
    in_specs = (
        rows, P("sp", None), P("sp", None), P("sp", None, None), P("sp", None, "tp"),
        P("sp", None, "tp"), P("sp", "tp", None), rows, rows, rows, rows, P(None, "tp"), P(None, "tp"),
    )
    out_specs = (
        rows, rows, rows, rows, rows, P("sp", None, "tp"), P("sp", None, "tp"), P("sp", "tp", None),
    )
    return jax.shard_map(
        per_device, mesh=mesh, in_specs=in_specs, out_specs=out_specs, check_vma=False
    )
```

```python
import functools
import math

import jax
import jax.numpy as jnp
from jax import lax
from jax.experimental import pallas as pl
from jax.experimental.pallas import tpu as pltpu
from jax.sharding import PartitionSpec as P

BF = jnp.bfloat16
F32 = jnp.float32
MESH = pl.DeviceIdType.MESH
VMEM = pl.BlockSpec(memory_space=pltpu.VMEM)
HBM = pl.BlockSpec(memory_space=pltpu.HBM)
NN = ((1,), (0,))


def dot(left, right, dims):
    return lax.dot_general(left, right, (dims, ((), ())), preferred_element_type=F32)


def remote(src, dst, send, recv, device):
    return pltpu.make_async_remote_copy(
        src_ref=src, dst_ref=dst, send_sem=send, recv_sem=recv, device_id=device, device_id_type=MESH
    )


def span(index, size):
    return pl.ds(pl.multiple_of(index * size, size), size)


def flip(s, m, n):
    out, bit = 0, 1
    while bit < n:
        out = out + bit * lax.rem(lax.div(s, bit) + (m // bit if isinstance(m, int) else lax.div(m, bit)), 2)
        bit *= 2
    return out


def low(m):
    return m & -m


def layer_kernel(
    n_sp, n_tp, experts, slot_scale,
    grad_hbm, ids_hbm, rw_hbm, x_hbm, gw_hbm, uw_hbm, dw_hbm,
    og_hbm, ig_hbm, val_hbm, conv_hbm, taps_hbm, pw_hbm,
    resid, og_out, ig_out, val_out, columns, zall, ggrad, ugrad, dgrad,
    grad, ids, rw, x, og, ig, val, conv, taps, pw,
    wt, dt, pre, routed, hidden, dall, outgoing, parts, from_sib, far_out, far_in, total, final, back, disp,
    rfull, pieces, edge_out, edge_in,
    load_sems, send_sems, ex_recv, q_recv, sib_recv, far_recv, misc_recv, gat_sems, z_recv, e_recv,
    halo_sems,
):
    me, tp = lax.axis_index("sp"), lax.axis_index("tp")
    core = lax.rem(tp, 2)
    sib = tp + 1 - 2 * core
    far = lax.rem(tp + n_tp // 2, n_tp)
    far_sib = lax.rem(sib + n_tp // 2, n_tp)
    tokens, chan = grad.shape
    slots, width = x.shape
    hid = dgrad.shape[1]
    cap = slots // n_sp
    half, quarter = n_sp // 2, n_sp // 4
    piece = width // n_sp
    per_block = chan // piece
    share = tokens // 2
    tile = 256

    pairs = [
        (grad_hbm, grad), (ids_hbm, ids), (rw_hbm, rw), (og_hbm, og), (conv_hbm, conv),
        (x_hbm.at[0], x), (gw_hbm, ggrad), (uw_hbm, ugrad), (dw_hbm, dgrad), (ig_hbm, ig), (val_hbm, val), (taps_hbm, taps), (pw_hbm, pw),
    ]
    loads = [pltpu.make_async_copy(a, b, load_sems.at[i]) for i, (a, b) in enumerate(pairs)]
    for load in loads[:3]:
        load.start()
    barrier = pltpu.get_barrier_semaphore()
    for m in range(1, n_sp):
        pl.semaphore_signal(barrier, inc=1, device_id={"sp": flip(me, m, n_sp)}, device_id_type=MESH)
    for other in (sib, far):
        pl.semaphore_signal(barrier, inc=1, device_id={"tp": other}, device_id_type=MESH)
    for load in loads[3:]:
        load.start()
    for load in loads[:3]:
        load.wait()

    id0, id1 = ids[0:1, :], ids[1:2, :]
    names = lax.broadcasted_iota(jnp.int32, (experts, tokens), 0)
    hit0 = jnp.where(id0 == names, 1.0, 0.0).astype(F32)
    hit1 = jnp.where(id1 == names, 1.0, 0.0).astype(F32)
    rows = lax.broadcasted_iota(jnp.int32, (tokens, tokens), 0)
    cols = lax.broadcasted_iota(jnp.int32, (tokens, tokens), 1)
    earlier = jnp.where(rows < cols, 1.0, 0.0).astype(BF)
    counts = dot((hit0 + hit1).astype(BF), earlier, NN)
    slot0 = id0.astype(F32) * float(cap) + jnp.sum(counts * hit0, axis=0, keepdims=True)
    slot1 = id1.astype(F32) * float(cap) + jnp.sum(counts * hit1, axis=0, keepdims=True)
    places = lax.broadcasted_iota(jnp.int32, (experts * cap, tokens), 0).astype(F32)
    at0, at1 = slot0 == places, slot1 == places
    weight = jnp.sum(
        jnp.where(at0, rw[0:1, :], 0.0) + jnp.where(at1, rw[1:2, :], 0.0), axis=1, keepdims=True
    )
    chosen = (jnp.where(at0, 1.0, 0.0) + jnp.where(at1, 1.0, 0.0)).astype(BF)
    outgoing[...] = (dot(chosen, grad[...], NN) * weight).astype(BF)

    pl.semaphore_wait(barrier, n_sp + 1)

    def row_at(s):
        return span(s, cap)

    def place(j, s):
        return routed.at[row_at(s), span(j, chan)]

    def sent(i, ref):
        return remote(ref, ref, send_sems.at[i], q_recv.at[0, 0], {"tp": sib})

    def taken(ref, sem):
        return remote(ref, ref, send_sems.at[0], sem, {"tp": sib})

    def sp_copy(m):
        to = flip(me, m, n_sp)
        return remote(
            outgoing.at[row_at(to), :], place(tp, me), send_sems.at[0], ex_recv.at[0, m], {"sp": to}
        )

    def far_share(m):
        at = place(tp, flip(me, m, n_sp))
        return remote(at, at, send_sems.at[1], ex_recv.at[1, m], {"tp": far})

    def sib_share(m):
        at = place(tp, flip(me, m, n_sp))
        return remote(at, at, send_sems.at[2], q_recv.at[0, lax.div(m, quarter)], {"tp": sib})

    def hand_share(m):
        at = place(far, flip(me, m, n_sp))
        return remote(at, at, send_sems.at[3], q_recv.at[1, lax.div(m, quarter)], {"tp": sib})

    def spread(m):
        sp_copy(m).wait_recv()
        far_share(m).start()
        sib_share(m).start()

    def hand(m):
        far_share(m).wait_recv()
        hand_share(m).start()

    @pl.loop(1, n_sp)
    def _(m):
        sp_copy(m).start()

    own = pltpu.make_async_copy(outgoing.at[row_at(me), :], place(tp, me), ex_recv.at[0, 0])
    own.start()
    own.wait()
    far_share(jnp.int32(0)).start()
    sib_share(jnp.int32(0)).start()

    loads[3].wait()
    loads[4].wait()
    zall[me] = (og[...].astype(F32) * conv[...].astype(F32)).astype(BF)
    disp[...] = chosen.T

    def z_copy(result, bit):
        block = flip(me, result - bit, n_sp)
        return remote(
            zall.at[block], zall.at[block], send_sems.at[7], z_recv.at[result],
            {"sp": flip(me, bit, n_sp)},
        )

    def z_send(m):
        bit = low(m) // 2 if m else half
        while bit:
            z_copy(m + bit, bit).start()
            bit //= 2

    def z_forward(m):
        if low(m) > 1:
            z_copy(m, low(m)).wait_recv()
            z_send(m)

    def pre_dot(t):
        at, up_at = span(t, tile), pl.ds(pl.multiple_of(hid + t * tile, tile), tile)
        pre[:, at] = dot(x[...], ggrad[0, :, at], NN)
        pre[:, up_at] = dot(x[...], ugrad[0, :, at], NN)

    for load in loads[6:8]:
        load.wait()
    def turn(i):
        at = span(i, tile)
        wt[:hid, at] = ggrad[0, at, :].T
        wt[hid:, at] = ugrad[0, at, :].T

    pre_tiles = hid // tile

    def prepare(t):
        pre_dot(t)
        dt[:, span(t, tile)] = dgrad[0, span(t, tile), :].T

    def each(lo, hi, step):
        if lo < hi:
            pl.loop(lo, hi)(step)

    bit, last = quarter // 2, half + quarter
    each(0, width // tile, turn)
    for load in (loads[5], loads[8]):
        load.wait()
    each(1, quarter, spread)
    each(0, min(1, pre_tiles), prepare)
    each(quarter, half, spread)
    each(0, bit, hand)
    each(1, min(2, pre_tiles), prepare)
    each(bit, quarter, hand)
    each(half, half + bit, spread)
    each(2, pre_tiles, prepare)
    each(quarter, quarter + bit, hand)
    each(half + bit, last, spread)
    each(quarter + bit, half, hand)

    def hidden_group(at):
        d_hidden = dot(routed[at, :], dt[...], NN)
        gate, up = pre[at, :hid], pre[at, hid:]
        sig = jax.nn.sigmoid(gate)
        act = gate * sig
        hidden[at, :] = (act * up).astype(BF)
        dall[at, :hid] = (d_hidden * up * sig * (1.0 + gate * (1.0 - sig))).astype(BF)
        dall[at, hid:] = (d_hidden * act).astype(BF)

    def arrived(q):
        for i in range(2):
            taken(outgoing.at[pl.ds(0, quarter * cap), :], q_recv.at[i, q]).wait_recv()

    near = span(lax.div(me, half), half * cap)
    fars = [span(flip(lax.div(me, quarter), 2 + i, 4), quarter * cap) for i in range(2)]
    group = [*fars, near]
    arrived(0)
    arrived(1)
    hidden_group(near)
    z_send(0)
    each(half, last, hand)
    each(last, last + bit, spread)

    def back_part(at, block, out):
        parts[out, at, :] = dot(dall[at, :], wt[:, span(block, chan)], NN).astype(BF)

    def sib_copy(g, i):
        return remote(
            parts.at[2 * i, group[g], :], from_sib.at[i, group[g], :],
            send_sems.at[4], sib_recv.at[2 * g + i], {"tp": sib},
        )

    side = chan // 2
    sides = [pl.ds(0, side), pl.ds(side, side)]

    def far_copy(m, h):
        at = row_at(flip(me, m, n_sp))
        return remote(
            far_out.at[at, sides[h]], far_in.at[at, sides[h]],
            send_sems.at[5], far_recv.at[h, m], {"tp": far},
        )

    def ret_copy(m, h):
        to = flip(me, m, n_sp)
        return remote(
            final.at[row_at(to), sides[h]], back.at[row_at(me), sides[h]],
            send_sems.at[6], misc_recv.at[h], {"sp": to},
        )

    def parts_of(g, i, others):
        for j in range(2):
            back_part(group[g], others[j], 2 * i + j)
            if j == 0:
                sib_copy(g, i).start()

    def push(m, h):
        r, c = row_at(flip(me, m, n_sp)), sides[h]
        far_out[r, c] = (parts[1, r, c].astype(F32) + from_sib[0, r, c].astype(F32)).astype(BF)
        far_copy(m, h).start()

    push0, push1 = (functools.partial(push, h=h) for h in range(2))

    def add_up(g):
        at = group[g]
        sib_copy(g, 1).wait_recv()
        total[at, :] = parts[3, at, :].astype(F32) + from_sib[1, at, :].astype(F32)

    def summed(r, h):
        return (total[r, sides[h]] + far_in[r, sides[h]].astype(F32)).astype(BF)

    def give(m, h):
        r = row_at(flip(me, m, n_sp))
        far_copy(m, h).wait_recv()
        final[r, sides[h]] = summed(r, h)
        ret_copy(m, h).start()

    give0, give1 = (functools.partial(give, h=h) for h in range(2))

    away_parts, home_parts = (far_sib, far), (sib, tp)
    arrived(2)
    hidden_group(fars[0])
    each(last + bit, n_sp, spread)
    parts_of(0, 0, away_parts)
    sib_copy(0, 0).wait_recv()
    each(half, last, push0)
    each(half, last, push1)
    parts_of(0, 1, home_parts)
    each(last, last + bit, hand)
    parts_of(2, 0, away_parts)
    each(last + bit, n_sp, hand)
    sib_copy(2, 0).wait_recv()
    each(1, half, push0)
    add_up(0)
    arrived(3)
    hidden_group(fars[1])
    each(half, last, give0)
    parts_of(1, 0, away_parts)
    each(half, last, give1)
    sib_copy(1, 0).wait_recv()
    each(last, n_sp, push0)
    push0(0)
    each(last, n_sp, push1)
    each(1, half, push1)
    push1(0)
    for m in range(1, half):
        z_forward(m)
    parts_of(1, 1, home_parts)
    parts_of(2, 1, home_parts)
    add_up(2)
    add_up(1)

    chunks = width // tile
    count = -(-chunks // half)

    def in_chunk(i):
        at = span(i, tile)
        left = x[:, at].T
        ggrad[0, at, :] = (dot(left, dall[:, :hid], NN) * slot_scale).astype(BF)
        ugrad[0, at, :] = (dot(left, dall[:, hid:], NN) * slot_scale).astype(BF)

    def fill(i):
        for j in range(count):
            c = i * count + j
            if count * half > chunks:
                pl.when(c < chunks)(functools.partial(in_chunk, c))
            else:
                in_chunk(c)

    def keep(h):
        r0 = row_at(me)
        far_copy(0, h).wait_recv()
        back[r0, sides[h]] = summed(r0, h)

    each(1, half, give0)
    fill(0)
    each(last, n_sp, give0)
    keep(0)
    fill(1)
    each(last, n_sp, give1)
    each(2, half - 1, fill)
    each(1, half, give1)
    keep(1)
    z_forward(half)
    fill(half - 1)

    for load in loads[9:]:
        load.wait()

    mine = span(core, share)

    def copy_block(block, h, i, other):
        ref = rfull.at[block, :, sides[h]]
        return remote(ref, ref, gat_sems.at[0, 3 * h + i], gat_sems.at[1, 3 * h + i], {"tp": other})

    away = [copy_block(tp, h, 0, far) for h in range(2)]
    close = [copy_block(tp, h, 1, sib) for h in range(2)]
    passed = [copy_block(far, h, 2, sib) for h in range(2)]

    def e_copy(k, m):
        return remote(pieces.at[k], columns.at[me, core], send_sems.at[8], e_recv.at[m], {"sp": k})

    def send_pieces(block, h):
        for j in range(h * per_block // 2, (h + 1) * per_block // 2):
            k = block * per_block + j
            pieces[k] = rfull[block, mine, pl.ds(j * piece, piece)]

            @pl.when(k != me)
            def _():
                e_copy(k, flip(me, k, n_sp)).start()

    def combine(h):
        c = sides[h]
        taken(outgoing.at[pl.ds(0, (n_sp - 1) * cap), c], misc_recv.at[h]).wait_recv()
        value = (grad[:, c].astype(F32) + dot(disp[...], back[:, c], NN)).astype(BF)
        resid[:, c] = value
        rfull[tp, :, c] = value
        away[h].start()
        close[h].start()
        send_pieces(tp, h)

    def mix_part(block):
        return dot(rfull[block], pw[span(block, chan), :], NN)

    def down_chunk(t):
        at = span(t, tile)
        dgrad[0, at, :] = (dot(hidden[:, at].T, routed[...], NN) * slot_scale).astype(BF)

    combine(0)
    pl.loop(0, hid // tile)(down_chunk)
    close[0].wait_recv()
    send_pieces(sib, 0)
    combine(1)
    mix = mix_part(tp)
    away[0].wait_recv()
    passed[0].start()
    send_pieces(far, 0)
    passed[0].wait_recv()
    send_pieces(far_sib, 0)
    for m in range(half + 1, n_sp):
        z_forward(m)
    close[1].wait_recv()
    send_pieces(sib, 1)
    mix = mix + mix_part(sib)
    away[1].wait_recv()
    passed[1].start()
    send_pieces(far, 1)
    mix = mix + mix_part(far)
    passed[1].wait_recv()
    send_pieces(far_sib, 1)
    mix = mix + mix_part(far_sib)
    for j in range(per_block):
        @pl.when(lax.rem(me, per_block) == j)
        def _():
            for c in range(2):
                columns[me, c] = rfull[
                    lax.div(me, per_block), pl.ds(c * share, share), pl.ds(j * piece, piece)
                ]

    conv_grad = (mix * og[...].astype(F32)).astype(BF).astype(F32)
    edge_out[0] = jnp.broadcast_to(conv_grad[tokens - 1:tokens, :], edge_out.shape[1:])
    edge_out[1] = jnp.broadcast_to(conv_grad[0:1, :], edge_out.shape[1:])
    ends = [lax.rem(me + 1, n_sp), lax.rem(me + n_sp - 1, n_sp)]
    halos = [
        remote(edge_out.at[i], edge_in.at[i], halo_sems.at[0, i], halo_sems.at[1, i], {"sp": ends[i]})
        for i in range(2)
    ]
    for halo in halos:
        halo.start()
    og_out[...] = (mix * conv[...].astype(F32)).astype(BF)

    def e_share(m):
        at = columns.at[flip(me, m, n_sp), core]
        return remote(at, at, send_sems.at[9], misc_recv.at[2], {"tp": sib})

    @pl.loop(1, n_sp)
    def _(m):
        e_copy(flip(me, m, n_sp), m).wait_recv()
        e_share(m).start()

    for halo in halos:
        halo.wait()
    before = jnp.where(me == 0, 0.0, edge_in[0, 0:1, :])
    after = jnp.where(me == n_sp - 1, 0.0, edge_in[1, 0:1, :])
    row = lax.broadcasted_iota(jnp.int32, (tokens, chan), 0)
    prev = jnp.where(row == 0, before, pltpu.roll(conv_grad, 1, 0))
    following = jnp.where(row == tokens - 1, after, pltpu.roll(conv_grad, tokens - 1, 0))
    tap = taps[...].astype(F32)
    value_grad = following * tap[0:1, :] + conv_grad * tap[1:2, :] + prev * tap[2:3, :]
    ig_out[...] = (value_grad * val[...].astype(F32)).astype(BF)
    val_out[...] = (value_grad * ig[...].astype(F32)).astype(BF)

    less = outgoing.at[pl.ds(0, (n_sp - 1) * cap), :]
    block = columns.at[pl.ds(0, n_sp - 1), 0]
    slices = [
        less, outgoing, outgoing, outgoing, from_sib, outgoing, less,
        zall.at[pl.ds(0, n_sp - 1)], pieces.at[pl.ds(0, n_sp - 1)], block,
    ]
    for i, ref in enumerate(slices):
        sent(i, ref).wait_send()
    taken(block, misc_recv.at[2]).wait_recv()
    for m in range(1, n_sp, 2):
        z_copy(m, 1).wait_recv()
    for copy in (*away, *close, *passed):
        copy.wait_send()


def finish_kernel(scale, columns, zall, *refs):
    grads, outs, proj, stage, sems = refs[:7], refs[7:14], refs[14], refs[15], refs[16]
    copies = [pltpu.make_async_copy(a, b, sems.at[i]) for i, (a, b) in enumerate(zip(grads, outs))]
    for copy in copies:
        copy.start()
    n_sp, parts, share, piece = columns.shape
    tokens = n_sp * parts * share
    left = columns[...].reshape(tokens, piece).T
    stage[...] = dot(left, zall[...].reshape(tokens, zall.shape[2]), NN) * scale
    last = pltpu.make_async_copy(stage, proj, sems.at[7])
    last.start()
    for copy in copies:
        copy.wait()
    last.wait()


def per_device(
    out_grad, route_ids, route_weight, expert_inputs, gate_weight, up_weight, down_weight,
    out_gate, in_gate, values, conv_out, conv_taps, proj_weight,
):
    n_sp, n_tp = lax.axis_size("sp"), lax.axis_size("tp")
    tokens, chan = out_grad.shape
    local, slots, width = expert_inputs.shape
    hid = gate_weight.shape[2]
    assert local == 1 and n_tp == 4 and n_sp & (n_sp - 1) == 0
    piece = width // n_sp
    dma = pltpu.SemaphoreType.DMA
    rows = jax.ShapeDtypeStruct((tokens, chan), BF)
    wide = jax.ShapeDtypeStruct((1, width, hid), BF)
    tall = jax.ShapeDtypeStruct((1, hid, width), BF)
    small = pltpu.VMEM((tokens, chan), BF)
    slab = pltpu.VMEM((slots, chan), BF)

    resid, og_out, ig_out, val_out, columns, zall, ggrad, ugrad, dgrad = pl.pallas_call(
        functools.partial(layer_kernel, n_sp, n_tp, n_sp * local, 1.0 / math.sqrt(slots)),
        out_shape=[
            rows, rows, rows, rows,
            jax.ShapeDtypeStruct((n_sp, 2, tokens // 2, piece), BF),
            jax.ShapeDtypeStruct((n_sp, tokens, chan), BF),
            wide, wide, tall,
        ],
        in_specs=[HBM] * 13,
        out_specs=[VMEM] * 9,
        scratch_shapes=[
            small,
            pltpu.VMEM((2, tokens), jnp.int32),
            pltpu.VMEM((2, tokens), F32),
            pltpu.VMEM((slots, width), BF),
            small, small, small, small,
            pltpu.VMEM(conv_taps.shape, BF),
            pltpu.VMEM(proj_weight.shape, BF),
            pltpu.VMEM((2 * hid, width), BF),
            pltpu.VMEM((width, hid), BF),
            pltpu.VMEM((slots, 2 * hid), F32),
            pltpu.VMEM((slots, width), BF),
            pltpu.VMEM((slots, hid), BF),
            pltpu.VMEM((slots, 2 * hid), BF),
            slab,
            pltpu.VMEM((4, slots, chan), BF),
            pltpu.VMEM((2, slots, chan), BF),
            slab, slab,
            pltpu.VMEM((slots, chan), F32),
            slab, slab,
            pltpu.VMEM((tokens, slots), BF),
            pltpu.VMEM((n_tp, tokens, chan), BF),
            pltpu.VMEM((n_sp, tokens // 2, piece), BF),
            pltpu.VMEM((2, 8, chan), F32),
            pltpu.VMEM((2, 8, chan), F32),
            dma((13,)), dma((10,)), dma((2, n_sp)), dma((2, 4)), dma((6,)), dma((2, n_sp)), dma((3,)),
            dma((2, 6)), dma((n_sp,)), dma((n_sp,)), dma((2, 2)),
        ],
        compiler_params=pltpu.CompilerParams(
            collective_id=0, has_side_effects=True, vmem_limit_bytes=38 * 2**20
        ),
        name="layer",
    )(*(
        pltpu.with_memory_space_constraint(a, pltpu.HBM) for a in (
            out_grad, route_ids.T, route_weight.T, expert_inputs, gate_weight, up_weight, down_weight,
            out_gate, in_gate, values, conv_out, conv_taps, proj_weight,
        )
    ))
    resid, og_out, ig_out, val_out, ggrad, ugrad, dgrad, proj_grad = pl.pallas_call(
        functools.partial(finish_kernel, 1.0 / math.sqrt(tokens * n_sp)),
        out_shape=[rows, rows, rows, rows, wide, wide, tall, jax.ShapeDtypeStruct((piece, chan), F32)],
        in_specs=[VMEM] * 9,
        out_specs=[HBM] * 8,
        scratch_shapes=[pltpu.VMEM((piece, chan), F32), dma((8,))],
        compiler_params=pltpu.CompilerParams(vmem_limit_bytes=6 * 2**20),
        name="finish",
    )(columns, zall, resid, og_out, ig_out, val_out, ggrad, ugrad, dgrad)
    return resid, og_out, ig_out, val_out, proj_grad, ggrad, ugrad, dgrad


def solution(mesh):
    rows = P("sp", "tp")
    in_specs = (
        rows, P("sp", None), P("sp", None), P("sp", None, None), P("sp", None, "tp"),
        P("sp", None, "tp"), P("sp", "tp", None), rows, rows, rows, rows, P(None, "tp"), P(None, "tp"),
    )
    out_specs = (
        rows, rows, rows, rows, rows, P("sp", None, "tp"), P("sp", None, "tp"), P("sp", "tp", None),
    )
    return jax.shard_map(
        per_device, mesh=mesh, in_specs=in_specs, out_specs=out_specs, check_vma=False
    )
```

```python
import functools
import math

import jax
import jax.numpy as jnp
from jax import lax
from jax.experimental import pallas as pl
from jax.experimental.pallas import tpu as pltpu
from jax.sharding import PartitionSpec as P

BF = jnp.bfloat16
F32 = jnp.float32
MESH = pl.DeviceIdType.MESH
VMEM = pl.BlockSpec(memory_space=pltpu.VMEM)
HBM = pl.BlockSpec(memory_space=pltpu.HBM)
NN = ((1,), (0,))


def dot(left, right, dims):
    return lax.dot_general(left, right, (dims, ((), ())), preferred_element_type=F32)


def remote(src, dst, send, recv, device):
    return pltpu.make_async_remote_copy(
        src_ref=src, dst_ref=dst, send_sem=send, recv_sem=recv, device_id=device, device_id_type=MESH
    )


def span(index, size):
    return pl.ds(pl.multiple_of(index * size, size), size)


def flip(s, m, n):
    out, bit = 0, 1
    while bit < n:
        out = out + bit * lax.rem(lax.div(s, bit) + (m // bit if isinstance(m, int) else lax.div(m, bit)), 2)
        bit *= 2
    return out


def low(m):
    return m & -m


def layer_kernel(
    n_sp, n_tp, experts, slot_scale,
    grad_hbm, ids_hbm, rw_hbm, x_hbm, gw_hbm, uw_hbm, dw_hbm,
    og_hbm, ig_hbm, val_hbm, conv_hbm, taps_hbm, pw_hbm,
    resid, og_out, ig_out, val_out, columns, zall, ggrad, ugrad, dgrad,
    grad, ids, rw, x, og, ig, val, conv, taps, pw,
    wt, dt, pre, routed, hidden, dall, outgoing, parts, from_sib, far_out, far_in, total, final, back, disp,
    rfull, pieces, edge_out, edge_in,
    load_sems, send_sems, ex_recv, q_recv, sib_recv, far_recv, misc_recv, gat_sems, z_recv, e_recv,
    halo_sems,
):
    me, tp = lax.axis_index("sp"), lax.axis_index("tp")
    core = lax.rem(tp, 2)
    sib = tp + 1 - 2 * core
    far = lax.rem(tp + n_tp // 2, n_tp)
    far_sib = lax.rem(sib + n_tp // 2, n_tp)
    tokens, chan = grad.shape
    slots, width = x.shape
    hid = dgrad.shape[1]
    cap = slots // n_sp
    half, quarter = n_sp // 2, n_sp // 4
    piece = width // n_sp
    per_block = chan // piece
    share = tokens // 2
    tile = 256

    pairs = [
        (grad_hbm, grad), (ids_hbm, ids), (rw_hbm, rw), (gw_hbm, ggrad), (uw_hbm, ugrad),
        (x_hbm.at[0], x), (dw_hbm, dgrad), (og_hbm, og), (conv_hbm, conv),
        (ig_hbm, ig), (val_hbm, val), (taps_hbm, taps), (pw_hbm, pw),
    ]
    loads = [pltpu.make_async_copy(a, b, load_sems.at[i]) for i, (a, b) in enumerate(pairs)]
    for load in loads[:3]:
        load.start()
    barrier = pltpu.get_barrier_semaphore()
    for m in range(1, n_sp):
        pl.semaphore_signal(barrier, inc=1, device_id={"sp": flip(me, m, n_sp)}, device_id_type=MESH)
    for other in (sib, far):
        pl.semaphore_signal(barrier, inc=1, device_id={"tp": other}, device_id_type=MESH)
    for load in loads[3:]:
        load.start()
    for load in loads[:3]:
        load.wait()

    id0, id1 = ids[0:1, :], ids[1:2, :]
    names = lax.broadcasted_iota(jnp.int32, (experts, tokens), 0)
    hit0 = jnp.where(id0 == names, 1.0, 0.0).astype(F32)
    hit1 = jnp.where(id1 == names, 1.0, 0.0).astype(F32)
    rows = lax.broadcasted_iota(jnp.int32, (tokens, tokens), 0)
    cols = lax.broadcasted_iota(jnp.int32, (tokens, tokens), 1)
    earlier = jnp.where(rows < cols, 1.0, 0.0).astype(BF)
    counts = dot((hit0 + hit1).astype(BF), earlier, NN)
    slot0 = id0.astype(F32) * float(cap) + jnp.sum(counts * hit0, axis=0, keepdims=True)
    slot1 = id1.astype(F32) * float(cap) + jnp.sum(counts * hit1, axis=0, keepdims=True)
    places = lax.broadcasted_iota(jnp.int32, (experts * cap, tokens), 0).astype(F32)
    at0, at1 = slot0 == places, slot1 == places
    weight = jnp.sum(
        jnp.where(at0, rw[0:1, :], 0.0) + jnp.where(at1, rw[1:2, :], 0.0), axis=1, keepdims=True
    )
    chosen = (jnp.where(at0, 1.0, 0.0) + jnp.where(at1, 1.0, 0.0)).astype(BF)
    outgoing[...] = (dot(chosen, grad[...], NN) * weight).astype(BF)

    pl.semaphore_wait(barrier, n_sp + 1)

    def row_at(s):
        return span(s, cap)

    def place(j, s):
        return routed.at[row_at(s), span(j, chan)]

    def sent(i, ref):
        return remote(ref, ref, send_sems.at[i], q_recv.at[0, 0], {"tp": sib})

    def taken(ref, sem):
        return remote(ref, ref, send_sems.at[0], sem, {"tp": sib})

    def sp_copy(m):
        to = flip(me, m, n_sp)
        return remote(
            outgoing.at[row_at(to), :], place(tp, me), send_sems.at[0], ex_recv.at[0, m], {"sp": to}
        )

    def far_share(m):
        at = place(tp, flip(me, m, n_sp))
        return remote(at, at, send_sems.at[1], ex_recv.at[1, m], {"tp": far})

    def sib_share(m):
        at = place(tp, flip(me, m, n_sp))
        return remote(at, at, send_sems.at[2], q_recv.at[0, lax.div(m, quarter)], {"tp": sib})

    def hand_share(m):
        at = place(far, flip(me, m, n_sp))
        return remote(at, at, send_sems.at[3], q_recv.at[1, lax.div(m, quarter)], {"tp": sib})

    def spread(m):
        sp_copy(m).wait_recv()
        far_share(m).start()
        sib_share(m).start()

    def hand(m):
        far_share(m).wait_recv()
        hand_share(m).start()

    def dispatch(m):
        sp_copy(m).start()

    last = half + quarter
    pl.loop(1, last)(dispatch)
    own = pltpu.make_async_copy(outgoing.at[row_at(me), :], place(tp, me), ex_recv.at[0, 0])
    own.start()
    own.wait()
    far_share(jnp.int32(0)).start()
    sib_share(jnp.int32(0)).start()

    disp[...] = chosen.T

    def z_copy(result, bit):
        block = flip(me, result - bit, n_sp)
        return remote(
            zall.at[block], zall.at[block], send_sems.at[7], z_recv.at[result],
            {"sp": flip(me, bit, n_sp)},
        )

    def z_send(m):
        bit = low(m) // 2 if m else half
        while bit:
            z_copy(m + bit, bit).start()
            bit //= 2

    def z_forward(m):
        if low(m) > 1:
            z_copy(m, low(m)).wait_recv()
            z_send(m)

    def pre_dot(t):
        at, up_at = span(t, tile), pl.ds(pl.multiple_of(hid + t * tile, tile), tile)
        pre[:, at] = dot(x[...], ggrad[0, :, at], NN)
        pre[:, up_at] = dot(x[...], ugrad[0, :, at], NN)

    for load in loads[3:5]:
        load.wait()
    def turn(i):
        at = span(i, tile)
        wt[:hid, at] = ggrad[0, at, :].T
        wt[hid:, at] = ugrad[0, at, :].T

    pre_tiles = hid // tile

    def prepare(t):
        pre_dot(t)
        dt[:, span(t, tile)] = dgrad[0, span(t, tile), :].T

    def each(lo, hi, step):
        if lo < hi:
            pl.loop(lo, hi)(step)

    bit = quarter // 2
    each(0, width // tile, turn)
    for load in loads[5:7]:
        load.wait()
    each(1, quarter, spread)
    each(0, min(1, pre_tiles), prepare)
    pl.loop(last, n_sp)(dispatch)
    each(quarter, half, spread)
    each(0, bit, hand)
    each(half, half + bit, spread)
    each(1, min(2, pre_tiles), prepare)
    each(bit, quarter, hand)
    each(half + bit, last, spread)
    each(quarter, quarter + bit, hand)
    each(2, pre_tiles, prepare)
    each(quarter + bit, half, hand)

    def hidden_group(at):
        d_hidden = dot(routed[at, :], dt[...], NN)
        gate, up = pre[at, :hid], pre[at, hid:]
        sig = jax.nn.sigmoid(gate)
        act = gate * sig
        hidden[at, :] = (act * up).astype(BF)
        dall[at, :hid] = (d_hidden * up * sig * (1.0 + gate * (1.0 - sig))).astype(BF)
        dall[at, hid:] = (d_hidden * act).astype(BF)

    def arrived(q):
        for i in range(2):
            taken(outgoing.at[pl.ds(0, quarter * cap), :], q_recv.at[i, q]).wait_recv()

    near = span(lax.div(me, half), half * cap)
    fars = [span(flip(lax.div(me, quarter), 2 + i, 4), quarter * cap) for i in range(2)]
    group = [*fars, near]
    arrived(0)
    arrived(1)
    hidden_group(near)
    for load in loads[7:9]:
        load.wait()
    zall[me] = (og[...].astype(F32) * conv[...].astype(F32)).astype(BF)
    z_send(0)
    each(half, last, hand)
    each(last, last + bit, spread)

    def back_part(at, block, out):
        parts[out, at, :] = dot(dall[at, :], wt[:, span(block, chan)], NN).astype(BF)

    def sib_copy(g, i):
        return remote(
            parts.at[2 * i, group[g], :], from_sib.at[i, group[g], :],
            send_sems.at[4], sib_recv.at[2 * g + i], {"tp": sib},
        )

    side = chan // 2
    sides = [pl.ds(0, side), pl.ds(side, side)]

    def far_copy(m, h):
        at = row_at(flip(me, m, n_sp))
        return remote(
            far_out.at[at, sides[h]], far_in.at[at, sides[h]],
            send_sems.at[5], far_recv.at[h, m], {"tp": far},
        )

    def ret_copy(m, h):
        to = flip(me, m, n_sp)
        return remote(
            final.at[row_at(to), sides[h]], back.at[row_at(me), sides[h]],
            send_sems.at[6], misc_recv.at[h], {"sp": to},
        )

    def parts_of(g, i, others):
        for j in range(2):
            back_part(group[g], others[j], 2 * i + j)
            if j == 0:
                sib_copy(g, i).start()

    def push(m, h):
        r, c = row_at(flip(me, m, n_sp)), sides[h]
        far_out[r, c] = (parts[1, r, c].astype(F32) + from_sib[0, r, c].astype(F32)).astype(BF)
        far_copy(m, h).start()

    push0, push1 = (functools.partial(push, h=h) for h in range(2))

    def add_up(g):
        at = group[g]
        sib_copy(g, 1).wait_recv()
        total[at, :] = parts[3, at, :].astype(F32) + from_sib[1, at, :].astype(F32)

    def summed(r, h):
        return (total[r, sides[h]] + far_in[r, sides[h]].astype(F32)).astype(BF)

    def give(m, h):
        r = row_at(flip(me, m, n_sp))
        far_copy(m, h).wait_recv()
        final[r, sides[h]] = summed(r, h)
        ret_copy(m, h).start()

    give0, give1 = (functools.partial(give, h=h) for h in range(2))

    away_parts, home_parts = (far_sib, far), (sib, tp)
    arrived(2)
    hidden_group(fars[0])
    each(last + bit, n_sp, spread)
    parts_of(0, 0, away_parts)
    sib_copy(0, 0).wait_recv()
    each(half, last, push0)
    each(half, last, push1)
    parts_of(0, 1, home_parts)
    each(last, last + bit, hand)
    parts_of(2, 0, away_parts)
    each(last + bit, n_sp, hand)
    sib_copy(2, 0).wait_recv()
    each(1, half, push0)
    add_up(0)
    arrived(3)
    hidden_group(fars[1])
    each(half, last, give0)
    parts_of(1, 0, away_parts)
    each(half, last, give1)
    sib_copy(1, 0).wait_recv()
    each(last, n_sp, push0)
    push0(0)
    each(last, n_sp, push1)
    each(1, half, push1)
    push1(0)
    for m in range(1, half):
        z_forward(m)
    parts_of(1, 1, home_parts)
    parts_of(2, 1, home_parts)
    add_up(2)
    add_up(1)

    chunks = width // tile
    count = -(-chunks // half)

    def in_chunk(i):
        at = span(i, tile)
        left = x[:, at].T
        ggrad[0, at, :] = (dot(left, dall[:, :hid], NN) * slot_scale).astype(BF)
        ugrad[0, at, :] = (dot(left, dall[:, hid:], NN) * slot_scale).astype(BF)

    def fill(i):
        for j in range(count):
            c = i * count + j
            if count * half > chunks:
                pl.when(c < chunks)(functools.partial(in_chunk, c))
            else:
                in_chunk(c)

    def keep(h):
        r0 = row_at(me)
        far_copy(0, h).wait_recv()
        back[r0, sides[h]] = summed(r0, h)

    each(1, half, give0)
    fill(0)
    each(last, n_sp, give0)
    keep(0)
    fill(1)
    each(last, n_sp, give1)
    each(2, half - 1, fill)
    each(1, half, give1)
    keep(1)
    z_forward(half)
    fill(half - 1)

    for load in loads[9:]:
        load.wait()

    mine = span(core, share)

    def copy_block(block, h, i, other):
        ref = rfull.at[block, :, sides[h]]
        return remote(ref, ref, gat_sems.at[0, 3 * h + i], gat_sems.at[1, 3 * h + i], {"tp": other})

    away = [copy_block(tp, h, 0, far) for h in range(2)]
    close = [copy_block(tp, h, 1, sib) for h in range(2)]
    passed = [copy_block(far, h, 2, sib) for h in range(2)]

    def e_copy(k, m):
        return remote(pieces.at[k], columns.at[me, core], send_sems.at[8], e_recv.at[m], {"sp": k})

    def send_pieces(block, h):
        for j in range(h * per_block // 2, (h + 1) * per_block // 2):
            k = block * per_block + j
            pieces[k] = rfull[block, mine, pl.ds(j * piece, piece)]

            @pl.when(k != me)
            def _():
                e_copy(k, flip(me, k, n_sp)).start()

    def combine(h):
        c = sides[h]
        taken(outgoing.at[pl.ds(0, (n_sp - 1) * cap), c], misc_recv.at[h]).wait_recv()
        value = (grad[:, c].astype(F32) + dot(disp[...], back[:, c], NN)).astype(BF)
        resid[:, c] = value
        rfull[tp, :, c] = value
        away[h].start()
        close[h].start()
        send_pieces(tp, h)

    def mix_part(block):
        return dot(rfull[block], pw[span(block, chan), :], NN)

    def down_chunk(t):
        at = span(t, tile)
        dgrad[0, at, :] = (dot(hidden[:, at].T, routed[...], NN) * slot_scale).astype(BF)

    combine(0)
    pl.loop(0, hid // tile)(down_chunk)
    close[0].wait_recv()
    send_pieces(sib, 0)
    combine(1)
    mix = mix_part(tp)
    away[0].wait_recv()
    passed[0].start()
    send_pieces(far, 0)
    for m in range(half + 1, n_sp):
        z_forward(m)
    passed[0].wait_recv()
    send_pieces(far_sib, 0)
    close[1].wait_recv()
    send_pieces(sib, 1)
    mix = mix + mix_part(sib)
    away[1].wait_recv()
    passed[1].start()
    send_pieces(far, 1)
    mix = mix + mix_part(far)
    passed[1].wait_recv()
    send_pieces(far_sib, 1)
    mix = mix + mix_part(far_sib)
    for j in range(per_block):
        @pl.when(lax.rem(me, per_block) == j)
        def _():
            for c in range(2):
                columns[me, c] = rfull[
                    lax.div(me, per_block), pl.ds(c * share, share), pl.ds(j * piece, piece)
                ]

    conv_grad = (mix * og[...].astype(F32)).astype(BF).astype(F32)
    edge_out[0] = jnp.broadcast_to(conv_grad[tokens - 1:tokens, :], edge_out.shape[1:])
    edge_out[1] = jnp.broadcast_to(conv_grad[0:1, :], edge_out.shape[1:])
    ends = [lax.rem(me + 1, n_sp), lax.rem(me + n_sp - 1, n_sp)]
    halos = [
        remote(edge_out.at[i], edge_in.at[i], halo_sems.at[0, i], halo_sems.at[1, i], {"sp": ends[i]})
        for i in range(2)
    ]
    for halo in halos:
        halo.start()
    og_out[...] = (mix * conv[...].astype(F32)).astype(BF)

    def e_share(m):
        at = columns.at[flip(me, m, n_sp), core]
        return remote(at, at, send_sems.at[9], misc_recv.at[2], {"tp": sib})

    @pl.loop(1, n_sp)
    def _(m):
        e_copy(flip(me, m, n_sp), m).wait_recv()
        e_share(m).start()

    for halo in halos:
        halo.wait()
    before = jnp.where(me == 0, 0.0, edge_in[0, 0:1, :])
    after = jnp.where(me == n_sp - 1, 0.0, edge_in[1, 0:1, :])
    row = lax.broadcasted_iota(jnp.int32, (tokens, chan), 0)
    prev = jnp.where(row == 0, before, pltpu.roll(conv_grad, 1, 0))
    following = jnp.where(row == tokens - 1, after, pltpu.roll(conv_grad, tokens - 1, 0))
    tap = taps[...].astype(F32)
    value_grad = following * tap[0:1, :] + conv_grad * tap[1:2, :] + prev * tap[2:3, :]
    ig_out[...] = (value_grad * val[...].astype(F32)).astype(BF)
    val_out[...] = (value_grad * ig[...].astype(F32)).astype(BF)

    less = outgoing.at[pl.ds(0, (n_sp - 1) * cap), :]
    block = columns.at[pl.ds(0, n_sp - 1), 0]
    slices = [
        less, outgoing, outgoing, outgoing, from_sib, outgoing, less,
        zall.at[pl.ds(0, n_sp - 1)], pieces.at[pl.ds(0, n_sp - 1)], block,
    ]
    for i, ref in enumerate(slices):
        sent(i, ref).wait_send()
    taken(block, misc_recv.at[2]).wait_recv()
    for m in range(1, n_sp, 2):
        z_copy(m, 1).wait_recv()
    for copy in (*away, *close, *passed):
        copy.wait_send()


def finish_kernel(scale, columns, zall, *refs):
    grads, outs, proj, stage, sems = refs[:7], refs[7:14], refs[14], refs[15], refs[16]
    copies = [pltpu.make_async_copy(a, b, sems.at[i]) for i, (a, b) in enumerate(zip(grads, outs))]
    cuts = 8
    for i in range(4, 7):
        rows = grads[i].shape[1] // cuts
        for c in range(cuts):
            at = pl.ds(c * rows, rows)
            pltpu.make_async_copy(grads[i].at[:, at], outs[i].at[:, at], sems.at[i]).start()
    for copy in copies[:4]:
        copy.start()
    n_sp, parts, share, piece = columns.shape
    tokens = n_sp * parts * share
    left = columns[...].reshape(tokens, piece).T
    stage[...] = dot(left, zall[...].reshape(tokens, zall.shape[2]), NN) * scale
    last = pltpu.make_async_copy(stage, proj, sems.at[7])
    last.start()
    for copy in copies:
        copy.wait()
    last.wait()


def per_device(
    out_grad, route_ids, route_weight, expert_inputs, gate_weight, up_weight, down_weight,
    out_gate, in_gate, values, conv_out, conv_taps, proj_weight,
):
    n_sp, n_tp = lax.axis_size("sp"), lax.axis_size("tp")
    tokens, chan = out_grad.shape
    local, slots, width = expert_inputs.shape
    hid = gate_weight.shape[2]
    assert local == 1 and n_tp == 4 and n_sp & (n_sp - 1) == 0
    piece = width // n_sp
    dma = pltpu.SemaphoreType.DMA
    rows = jax.ShapeDtypeStruct((tokens, chan), BF)
    wide = jax.ShapeDtypeStruct((1, width, hid), BF)
    tall = jax.ShapeDtypeStruct((1, hid, width), BF)
    small = pltpu.VMEM((tokens, chan), BF)
    slab = pltpu.VMEM((slots, chan), BF)

    resid, og_out, ig_out, val_out, columns, zall, ggrad, ugrad, dgrad = pl.pallas_call(
        functools.partial(layer_kernel, n_sp, n_tp, n_sp * local, 1.0 / math.sqrt(slots)),
        out_shape=[
            rows, rows, rows, rows,
            jax.ShapeDtypeStruct((n_sp, 2, tokens // 2, piece), BF),
            jax.ShapeDtypeStruct((n_sp, tokens, chan), BF),
            wide, wide, tall,
        ],
        in_specs=[HBM] * 13,
        out_specs=[VMEM] * 9,
        scratch_shapes=[
            small,
            pltpu.VMEM((2, tokens), jnp.int32),
            pltpu.VMEM((2, tokens), F32),
            pltpu.VMEM((slots, width), BF),
            small, small, small, small,
            pltpu.VMEM(conv_taps.shape, BF),
            pltpu.VMEM(proj_weight.shape, BF),
            pltpu.VMEM((2 * hid, width), BF),
            pltpu.VMEM((width, hid), BF),
            pltpu.VMEM((slots, 2 * hid), F32),
            pltpu.VMEM((slots, width), BF),
            pltpu.VMEM((slots, hid), BF),
            pltpu.VMEM((slots, 2 * hid), BF),
            slab,
            pltpu.VMEM((4, slots, chan), BF),
            pltpu.VMEM((2, slots, chan), BF),
            slab, slab,
            pltpu.VMEM((slots, chan), F32),
            slab, slab,
            pltpu.VMEM((tokens, slots), BF),
            pltpu.VMEM((n_tp, tokens, chan), BF),
            pltpu.VMEM((n_sp, tokens // 2, piece), BF),
            pltpu.VMEM((2, 8, chan), F32),
            pltpu.VMEM((2, 8, chan), F32),
            dma((13,)), dma((10,)), dma((2, n_sp)), dma((2, 4)), dma((6,)), dma((2, n_sp)), dma((3,)),
            dma((2, 6)), dma((n_sp,)), dma((n_sp,)), dma((2, 2)),
        ],
        compiler_params=pltpu.CompilerParams(
            collective_id=0, has_side_effects=True, vmem_limit_bytes=38 * 2**20
        ),
        name="layer",
    )(*(
        pltpu.with_memory_space_constraint(a, pltpu.HBM) for a in (
            out_grad, route_ids.T, route_weight.T, expert_inputs, gate_weight, up_weight, down_weight,
            out_gate, in_gate, values, conv_out, conv_taps, proj_weight,
        )
    ))
    resid, og_out, ig_out, val_out, ggrad, ugrad, dgrad, proj_grad = pl.pallas_call(
        functools.partial(finish_kernel, 1.0 / math.sqrt(tokens * n_sp)),
        out_shape=[rows, rows, rows, rows, wide, wide, tall, jax.ShapeDtypeStruct((piece, chan), F32)],
        in_specs=[VMEM] * 9,
        out_specs=[HBM] * 8,
        scratch_shapes=[pltpu.VMEM((piece, chan), F32), dma((8,))],
        compiler_params=pltpu.CompilerParams(vmem_limit_bytes=6 * 2**20),
        name="finish",
    )(columns, zall, resid, og_out, ig_out, val_out, ggrad, ugrad, dgrad)
    return resid, og_out, ig_out, val_out, proj_grad, ggrad, ugrad, dgrad


def solution(mesh):
    rows = P("sp", "tp")
    in_specs = (
        rows, P("sp", None), P("sp", None), P("sp", None, None), P("sp", None, "tp"),
        P("sp", None, "tp"), P("sp", "tp", None), rows, rows, rows, rows, P(None, "tp"), P(None, "tp"),
    )
    out_specs = (
        rows, rows, rows, rows, rows, P("sp", None, "tp"), P("sp", None, "tp"), P("sp", "tp", None),
    )
    return jax.shard_map(
        per_device, mesh=mesh, in_specs=in_specs, out_specs=out_specs, check_vma=False
    )
```

```python
import functools
import math

import jax
import jax.numpy as jnp
from jax import lax
from jax.experimental import pallas as pl
from jax.experimental.pallas import tpu as pltpu
from jax.sharding import PartitionSpec as P

BF = jnp.bfloat16
F32 = jnp.float32
MESH = pl.DeviceIdType.MESH
VMEM = pl.BlockSpec(memory_space=pltpu.VMEM)
HBM = pl.BlockSpec(memory_space=pltpu.HBM)
NN = ((1,), (0,))


def dot(left, right, dims):
    return lax.dot_general(left, right, (dims, ((), ())), preferred_element_type=F32)


def remote(src, dst, send, recv, device):
    return pltpu.make_async_remote_copy(
        src_ref=src, dst_ref=dst, send_sem=send, recv_sem=recv, device_id=device, device_id_type=MESH
    )


def span(index, size):
    return pl.ds(pl.multiple_of(index * size, size), size)


def flip(s, m, n):
    out, bit = 0, 1
    while bit < n:
        out = out + bit * lax.rem(lax.div(s, bit) + (m // bit if isinstance(m, int) else lax.div(m, bit)), 2)
        bit *= 2
    return out


def low(m):
    return m & -m


def layer_kernel(
    n_sp, n_tp, experts, slot_scale,
    grad_hbm, ids_hbm, rw_hbm, x_hbm, gw_hbm, uw_hbm, dw_hbm,
    og_hbm, ig_hbm, val_hbm, conv_hbm, taps_hbm, pw_hbm,
    resid, og_out, ig_out, val_out, columns, zall, ggrad, ugrad, dgrad,
    grad, ids, rw, x, og, ig, val, conv, taps, pw,
    wt, dt, pre, routed, hidden, dall, outgoing, parts, from_sib, far_out, far_in, total, final, back, disp,
    rfull, pieces, edge_out, edge_in,
    load_sems, send_sems, ex_recv, q_recv, sib_recv, far_recv, misc_recv, gat_sems, z_recv, e_recv,
    halo_sems,
):
    me, tp = lax.axis_index("sp"), lax.axis_index("tp")
    core = lax.rem(tp, 2)
    sib = tp + 1 - 2 * core
    far = lax.rem(tp + n_tp // 2, n_tp)
    far_sib = lax.rem(sib + n_tp // 2, n_tp)
    tokens, chan = grad.shape
    slots, width = x.shape
    hid = dgrad.shape[1]
    cap = slots // n_sp
    half, quarter = n_sp // 2, n_sp // 4
    piece = width // n_sp
    per_block = chan // piece
    share = tokens // 2
    tile = 256

    pairs = [
        (grad_hbm, grad), (ids_hbm, ids), (rw_hbm, rw), (gw_hbm, ggrad), (uw_hbm, ugrad),
        (x_hbm.at[0], x), (dw_hbm, dgrad), (og_hbm, og), (conv_hbm, conv),
        (ig_hbm, ig), (val_hbm, val), (taps_hbm, taps), (pw_hbm, pw),
    ]
    loads = [pltpu.make_async_copy(a, b, load_sems.at[i]) for i, (a, b) in enumerate(pairs)]
    for load in loads[:3]:
        load.start()
    barrier = pltpu.get_barrier_semaphore()
    for m in range(1, n_sp):
        pl.semaphore_signal(barrier, inc=1, device_id={"sp": flip(me, m, n_sp)}, device_id_type=MESH)
    for other in (sib, far):
        pl.semaphore_signal(barrier, inc=1, device_id={"tp": other}, device_id_type=MESH)
    for load in loads[3:]:
        load.start()
    for load in loads[:3]:
        load.wait()

    id0, id1 = ids[0:1, :], ids[1:2, :]
    names = lax.broadcasted_iota(jnp.int32, (experts, tokens), 0)
    hit0 = jnp.where(id0 == names, 1.0, 0.0).astype(F32)
    hit1 = jnp.where(id1 == names, 1.0, 0.0).astype(F32)
    rows = lax.broadcasted_iota(jnp.int32, (tokens, tokens), 0)
    cols = lax.broadcasted_iota(jnp.int32, (tokens, tokens), 1)
    earlier = jnp.where(rows < cols, 1.0, 0.0).astype(BF)
    counts = dot((hit0 + hit1).astype(BF), earlier, NN)
    slot0 = id0.astype(F32) * float(cap) + jnp.sum(counts * hit0, axis=0, keepdims=True)
    slot1 = id1.astype(F32) * float(cap) + jnp.sum(counts * hit1, axis=0, keepdims=True)
    places = lax.broadcasted_iota(jnp.int32, (experts * cap, tokens), 0).astype(F32)
    at0, at1 = slot0 == places, slot1 == places
    weight = jnp.sum(
        jnp.where(at0, rw[0:1, :], 0.0) + jnp.where(at1, rw[1:2, :], 0.0), axis=1, keepdims=True
    )
    chosen = (jnp.where(at0, 1.0, 0.0) + jnp.where(at1, 1.0, 0.0)).astype(BF)
    outgoing[...] = (dot(chosen, grad[...], NN) * weight).astype(BF)

    pl.semaphore_wait(barrier, n_sp + 1)

    def row_at(s):
        return span(s, cap)

    def place(j, s):
        return routed.at[row_at(s), span(j, chan)]

    def sent(i, ref):
        return remote(ref, ref, send_sems.at[i], q_recv.at[0, 0], {"tp": sib})

    def taken(ref, sem):
        return remote(ref, ref, send_sems.at[0], sem, {"tp": sib})

    def sp_copy(m):
        to = flip(me, m, n_sp)
        return remote(
            outgoing.at[row_at(to), :], place(tp, me), send_sems.at[0], ex_recv.at[0, m], {"sp": to}
        )

    def far_share(m):
        at = place(tp, flip(me, m, n_sp))
        return remote(at, at, send_sems.at[1], ex_recv.at[1, m], {"tp": far})

    def sib_share(m):
        at = place(tp, flip(me, m, n_sp))
        return remote(at, at, send_sems.at[2], q_recv.at[0, lax.div(m, quarter)], {"tp": sib})

    def hand_share(m):
        at = place(far, flip(me, m, n_sp))
        return remote(at, at, send_sems.at[3], q_recv.at[1, lax.div(m, quarter)], {"tp": sib})

    def spread(m):
        sp_copy(m).wait_recv()
        far_share(m).start()
        sib_share(m).start()

    def hand(m):
        far_share(m).wait_recv()
        hand_share(m).start()

    def dispatch(m):
        sp_copy(m).start()

    last = half + quarter
    pl.loop(1, last)(dispatch)
    own = pltpu.make_async_copy(outgoing.at[row_at(me), :], place(tp, me), ex_recv.at[0, 0])
    own.start()
    own.wait()
    far_share(jnp.int32(0)).start()
    sib_share(jnp.int32(0)).start()

    disp[...] = chosen.T

    def z_copy(result, bit):
        block = flip(me, result - bit, n_sp)
        return remote(
            zall.at[block], zall.at[block], send_sems.at[7], z_recv.at[result],
            {"sp": flip(me, bit, n_sp)},
        )

    def z_send(m):
        bit = low(m) // 2 if m else half
        while bit:
            z_copy(m + bit, bit).start()
            bit //= 2

    def z_forward(m):
        if low(m) > 1:
            z_copy(m, low(m)).wait_recv()
            z_send(m)

    def pre_dot(t):
        at, up_at = span(t, tile), pl.ds(pl.multiple_of(hid + t * tile, tile), tile)
        pre[:, at] = dot(x[...], ggrad[0, :, at], NN)
        pre[:, up_at] = dot(x[...], ugrad[0, :, at], NN)

    for load in loads[3:5]:
        load.wait()
    def turn(i):
        at = span(i, tile)
        wt[:hid, at] = ggrad[0, at, :].T
        wt[hid:, at] = ugrad[0, at, :].T

    pre_tiles = hid // tile

    def prepare(t):
        pre_dot(t)
        dt[:, span(t, tile)] = dgrad[0, span(t, tile), :].T

    def each(lo, hi, step):
        if lo < hi:
            pl.loop(lo, hi)(step)

    bit = quarter // 2
    each(0, width // tile, turn)
    for load in loads[5:7]:
        load.wait()
    each(1, quarter, spread)
    each(0, min(1, pre_tiles), prepare)
    each(quarter, half, spread)
    pl.loop(last, n_sp)(dispatch)
    each(0, bit, hand)
    each(half, half + bit, spread)
    each(1, min(2, pre_tiles), prepare)
    each(bit, quarter, hand)
    each(half + bit, last, spread)
    each(quarter, quarter + bit, hand)
    each(2, pre_tiles, prepare)
    each(quarter + bit, half, hand)

    def hidden_group(at):
        d_hidden = dot(routed[at, :], dt[...], NN)
        gate, up = pre[at, :hid], pre[at, hid:]
        sig = jax.nn.sigmoid(gate)
        act = gate * sig
        hidden[at, :] = (act * up).astype(BF)
        dall[at, :hid] = (d_hidden * up * sig * (1.0 + gate * (1.0 - sig))).astype(BF)
        dall[at, hid:] = (d_hidden * act).astype(BF)

    def arrived(q):
        for i in range(2):
            taken(outgoing.at[pl.ds(0, quarter * cap), :], q_recv.at[i, q]).wait_recv()

    near = span(lax.div(me, half), half * cap)
    fars = [span(flip(lax.div(me, quarter), 2 + i, 4), quarter * cap) for i in range(2)]
    group = [*fars, near]
    arrived(0)
    arrived(1)
    hidden_group(near)
    for load in loads[7:9]:
        load.wait()
    zall[me] = (og[...].astype(F32) * conv[...].astype(F32)).astype(BF)
    z_send(0)
    each(half, last, hand)
    each(last, last + bit, spread)

    def back_part(at, block, out):
        parts[out, at, :] = dot(dall[at, :], wt[:, span(block, chan)], NN).astype(BF)

    def sib_copy(g, i):
        return remote(
            parts.at[2 * i, group[g], :], from_sib.at[i, group[g], :],
            send_sems.at[4], sib_recv.at[2 * g + i], {"tp": sib},
        )

    side = chan // 2
    sides = [pl.ds(0, side), pl.ds(side, side)]

    def far_copy(m, h):
        at = row_at(flip(me, m, n_sp))
        return remote(
            far_out.at[at, sides[h]], far_in.at[at, sides[h]],
            send_sems.at[5], far_recv.at[h, m], {"tp": far},
        )

    def ret_copy(m, h):
        to = flip(me, m, n_sp)
        return remote(
            final.at[row_at(to), sides[h]], back.at[row_at(me), sides[h]],
            send_sems.at[6], misc_recv.at[h], {"sp": to},
        )

    def parts_of(g, i, others):
        for j in range(2):
            back_part(group[g], others[j], 2 * i + j)
            if j == 0:
                sib_copy(g, i).start()

    def push(m, h):
        r, c = row_at(flip(me, m, n_sp)), sides[h]
        far_out[r, c] = (parts[1, r, c].astype(F32) + from_sib[0, r, c].astype(F32)).astype(BF)
        far_copy(m, h).start()

    push0, push1 = (functools.partial(push, h=h) for h in range(2))

    def add_up(g):
        at = group[g]
        sib_copy(g, 1).wait_recv()
        total[at, :] = parts[3, at, :].astype(F32) + from_sib[1, at, :].astype(F32)

    def summed(r, h):
        return (total[r, sides[h]] + far_in[r, sides[h]].astype(F32)).astype(BF)

    def give(m, h):
        r = row_at(flip(me, m, n_sp))
        far_copy(m, h).wait_recv()
        final[r, sides[h]] = summed(r, h)
        ret_copy(m, h).start()

    give0, give1 = (functools.partial(give, h=h) for h in range(2))

    away_parts, home_parts = (far_sib, far), (sib, tp)
    arrived(2)
    hidden_group(fars[0])
    each(last + bit, n_sp, spread)
    parts_of(0, 0, away_parts)
    sib_copy(0, 0).wait_recv()
    each(half, last, push0)
    each(half, last, push1)
    parts_of(0, 1, home_parts)
    each(last, last + bit, hand)
    parts_of(2, 0, away_parts)
    each(last + bit, n_sp, hand)
    sib_copy(2, 0).wait_recv()
    each(1, half, push0)
    add_up(0)
    arrived(3)
    hidden_group(fars[1])
    each(half, last, give0)
    parts_of(1, 0, away_parts)
    each(half, last, give1)
    sib_copy(1, 0).wait_recv()
    each(last, n_sp, push0)
    push0(0)
    each(last, n_sp, push1)
    each(1, half, push1)
    push1(0)
    for m in range(1, half):
        z_forward(m)
    parts_of(1, 1, home_parts)
    parts_of(2, 1, home_parts)
    add_up(2)
    add_up(1)

    chunks = width // tile
    count = -(-chunks // half)

    def in_chunk(i):
        at = span(i, tile)
        left = x[:, at].T
        ggrad[0, at, :] = (dot(left, dall[:, :hid], NN) * slot_scale).astype(BF)
        ugrad[0, at, :] = (dot(left, dall[:, hid:], NN) * slot_scale).astype(BF)

    def fill(i):
        for j in range(count):
            c = i * count + j
            if count * half > chunks:
                pl.when(c < chunks)(functools.partial(in_chunk, c))
            else:
                in_chunk(c)

    def keep(h):
        r0 = row_at(me)
        far_copy(0, h).wait_recv()
        back[r0, sides[h]] = summed(r0, h)

    each(1, half, give0)
    fill(0)
    each(last, n_sp, give0)
    keep(0)
    fill(1)
    each(last, n_sp, give1)
    each(2, half - 1, fill)
    each(1, half, give1)
    keep(1)
    z_forward(half)
    fill(half - 1)

    for load in loads[9:]:
        load.wait()

    mine = span(core, share)

    def copy_block(block, h, i, other):
        ref = rfull.at[block, :, sides[h]]
        return remote(ref, ref, gat_sems.at[0, 3 * h + i], gat_sems.at[1, 3 * h + i], {"tp": other})

    away = [copy_block(tp, h, 0, far) for h in range(2)]
    close = [copy_block(tp, h, 1, sib) for h in range(2)]
    passed = [copy_block(far, h, 2, sib) for h in range(2)]

    def e_copy(k, m):
        return remote(pieces.at[k], columns.at[me, core], send_sems.at[8], e_recv.at[m], {"sp": k})

    def send_pieces(block, h):
        for j in range(h * per_block // 2, (h + 1) * per_block // 2):
            k = block * per_block + j
            pieces[k] = rfull[block, mine, pl.ds(j * piece, piece)]

            @pl.when(k != me)
            def _():
                e_copy(k, flip(me, k, n_sp)).start()

    def combine(h):
        c = sides[h]
        taken(outgoing.at[pl.ds(0, (n_sp - 1) * cap), c], misc_recv.at[h]).wait_recv()
        value = (grad[:, c].astype(F32) + dot(disp[...], back[:, c], NN)).astype(BF)
        resid[:, c] = value
        rfull[tp, :, c] = value
        away[h].start()
        close[h].start()
        send_pieces(tp, h)

    def mix_part(block):
        return dot(rfull[block], pw[span(block, chan), :], NN)

    def down_chunk(t):
        at = span(t, tile)
        dgrad[0, at, :] = (dot(hidden[:, at].T, routed[...], NN) * slot_scale).astype(BF)

    combine(0)
    pl.loop(0, hid // tile)(down_chunk)
    close[0].wait_recv()
    send_pieces(sib, 0)
    combine(1)
    mix = mix_part(tp)
    away[0].wait_recv()
    passed[0].start()
    send_pieces(far, 0)
    for m in range(half + 1, n_sp):
        z_forward(m)
    passed[0].wait_recv()
    send_pieces(far_sib, 0)
    close[1].wait_recv()
    send_pieces(sib, 1)
    mix = mix + mix_part(sib)
    away[1].wait_recv()
    passed[1].start()
    send_pieces(far, 1)
    mix = mix + mix_part(far)
    passed[1].wait_recv()
    send_pieces(far_sib, 1)
    mix = mix + mix_part(far_sib)
    for j in range(per_block):
        @pl.when(lax.rem(me, per_block) == j)
        def _():
            for c in range(2):
                columns[me, c] = rfull[
                    lax.div(me, per_block), pl.ds(c * share, share), pl.ds(j * piece, piece)
                ]

    conv_grad = (mix * og[...].astype(F32)).astype(BF).astype(F32)
    edge_out[0] = jnp.broadcast_to(conv_grad[tokens - 1:tokens, :], edge_out.shape[1:])
    edge_out[1] = jnp.broadcast_to(conv_grad[0:1, :], edge_out.shape[1:])
    ends = [lax.rem(me + 1, n_sp), lax.rem(me + n_sp - 1, n_sp)]
    halos = [
        remote(edge_out.at[i], edge_in.at[i], halo_sems.at[0, i], halo_sems.at[1, i], {"sp": ends[i]})
        for i in range(2)
    ]
    for halo in halos:
        halo.start()
    og_out[...] = (mix * conv[...].astype(F32)).astype(BF)

    def e_share(m):
        at = columns.at[flip(me, m, n_sp), core]
        return remote(at, at, send_sems.at[9], misc_recv.at[2], {"tp": sib})

    @pl.loop(1, n_sp)
    def _(m):
        e_copy(flip(me, m, n_sp), m).wait_recv()
        e_share(m).start()

    for halo in halos:
        halo.wait()
    before = jnp.where(me == 0, 0.0, edge_in[0, 0:1, :])
    after = jnp.where(me == n_sp - 1, 0.0, edge_in[1, 0:1, :])
    row = lax.broadcasted_iota(jnp.int32, (tokens, chan), 0)
    prev = jnp.where(row == 0, before, pltpu.roll(conv_grad, 1, 0))
    following = jnp.where(row == tokens - 1, after, pltpu.roll(conv_grad, tokens - 1, 0))
    tap = taps[...].astype(F32)
    value_grad = following * tap[0:1, :] + conv_grad * tap[1:2, :] + prev * tap[2:3, :]
    ig_out[...] = (value_grad * val[...].astype(F32)).astype(BF)
    val_out[...] = (value_grad * ig[...].astype(F32)).astype(BF)

    less = outgoing.at[pl.ds(0, (n_sp - 1) * cap), :]
    block = columns.at[pl.ds(0, n_sp - 1), 0]
    slices = [
        less, outgoing, outgoing, outgoing, from_sib, outgoing, less,
        zall.at[pl.ds(0, n_sp - 1)], pieces.at[pl.ds(0, n_sp - 1)], block,
    ]
    for i, ref in enumerate(slices):
        sent(i, ref).wait_send()
    taken(block, misc_recv.at[2]).wait_recv()
    for m in range(1, n_sp, 2):
        z_copy(m, 1).wait_recv()
    for copy in (*away, *close, *passed):
        copy.wait_send()


def finish_kernel(scale, columns, zall, *refs):
    grads, outs, proj, stage, sems = refs[:7], refs[7:14], refs[14], refs[15], refs[16]
    copies = [pltpu.make_async_copy(a, b, sems.at[i]) for i, (a, b) in enumerate(zip(grads, outs))]
    cuts = 8
    for i in range(4, 7):
        rows = grads[i].shape[1] // cuts
        for c in range(cuts):
            at = pl.ds(c * rows, rows)
            pltpu.make_async_copy(grads[i].at[:, at], outs[i].at[:, at], sems.at[i]).start()
    for copy in copies[:4]:
        copy.start()
    n_sp, parts, share, piece = columns.shape
    tokens = n_sp * parts * share
    left = columns[...].reshape(tokens, piece).T
    stage[...] = dot(left, zall[...].reshape(tokens, zall.shape[2]), NN) * scale
    last = pltpu.make_async_copy(stage, proj, sems.at[7])
    last.start()
    for copy in copies:
        copy.wait()
    last.wait()


def per_device(
    out_grad, route_ids, route_weight, expert_inputs, gate_weight, up_weight, down_weight,
    out_gate, in_gate, values, conv_out, conv_taps, proj_weight,
):
    n_sp, n_tp = lax.axis_size("sp"), lax.axis_size("tp")
    tokens, chan = out_grad.shape
    local, slots, width = expert_inputs.shape
    hid = gate_weight.shape[2]
    assert local == 1 and n_tp == 4 and n_sp & (n_sp - 1) == 0
    piece = width // n_sp
    dma = pltpu.SemaphoreType.DMA
    rows = jax.ShapeDtypeStruct((tokens, chan), BF)
    wide = jax.ShapeDtypeStruct((1, width, hid), BF)
    tall = jax.ShapeDtypeStruct((1, hid, width), BF)
    small = pltpu.VMEM((tokens, chan), BF)
    slab = pltpu.VMEM((slots, chan), BF)

    resid, og_out, ig_out, val_out, columns, zall, ggrad, ugrad, dgrad = pl.pallas_call(
        functools.partial(layer_kernel, n_sp, n_tp, n_sp * local, 1.0 / math.sqrt(slots)),
        out_shape=[
            rows, rows, rows, rows,
            jax.ShapeDtypeStruct((n_sp, 2, tokens // 2, piece), BF),
            jax.ShapeDtypeStruct((n_sp, tokens, chan), BF),
            wide, wide, tall,
        ],
        in_specs=[HBM] * 13,
        out_specs=[VMEM] * 9,
        scratch_shapes=[
            small,
            pltpu.VMEM((2, tokens), jnp.int32),
            pltpu.VMEM((2, tokens), F32),
            pltpu.VMEM((slots, width), BF),
            small, small, small, small,
            pltpu.VMEM(conv_taps.shape, BF),
            pltpu.VMEM(proj_weight.shape, BF),
            pltpu.VMEM((2 * hid, width), BF),
            pltpu.VMEM((width, hid), BF),
            pltpu.VMEM((slots, 2 * hid), F32),
            pltpu.VMEM((slots, width), BF),
            pltpu.VMEM((slots, hid), BF),
            pltpu.VMEM((slots, 2 * hid), BF),
            slab,
            pltpu.VMEM((4, slots, chan), BF),
            pltpu.VMEM((2, slots, chan), BF),
            slab, slab,
            pltpu.VMEM((slots, chan), F32),
            slab, slab,
            pltpu.VMEM((tokens, slots), BF),
            pltpu.VMEM((n_tp, tokens, chan), BF),
            pltpu.VMEM((n_sp, tokens // 2, piece), BF),
            pltpu.VMEM((2, 8, chan), F32),
            pltpu.VMEM((2, 8, chan), F32),
            dma((13,)), dma((10,)), dma((2, n_sp)), dma((2, 4)), dma((6,)), dma((2, n_sp)), dma((3,)),
            dma((2, 6)), dma((n_sp,)), dma((n_sp,)), dma((2, 2)),
        ],
        compiler_params=pltpu.CompilerParams(
            collective_id=0, has_side_effects=True, vmem_limit_bytes=38 * 2**20
        ),
        name="layer",
    )(*(
        pltpu.with_memory_space_constraint(a, pltpu.HBM) for a in (
            out_grad, route_ids.T, route_weight.T, expert_inputs, gate_weight, up_weight, down_weight,
            out_gate, in_gate, values, conv_out, conv_taps, proj_weight,
        )
    ))
    resid, og_out, ig_out, val_out, ggrad, ugrad, dgrad, proj_grad = pl.pallas_call(
        functools.partial(finish_kernel, 1.0 / math.sqrt(tokens * n_sp)),
        out_shape=[rows, rows, rows, rows, wide, wide, tall, jax.ShapeDtypeStruct((piece, chan), F32)],
        in_specs=[VMEM] * 9,
        out_specs=[HBM] * 8,
        scratch_shapes=[pltpu.VMEM((piece, chan), F32), dma((8,))],
        compiler_params=pltpu.CompilerParams(vmem_limit_bytes=6 * 2**20),
        name="finish",
    )(columns, zall, resid, og_out, ig_out, val_out, ggrad, ugrad, dgrad)
    return resid, og_out, ig_out, val_out, proj_grad, ggrad, ugrad, dgrad


def solution(mesh):
    rows = P("sp", "tp")
    in_specs = (
        rows, P("sp", None), P("sp", None), P("sp", None, None), P("sp", None, "tp"),
        P("sp", None, "tp"), P("sp", "tp", None), rows, rows, rows, rows, P(None, "tp"), P(None, "tp"),
    )
    out_specs = (
        rows, rows, rows, rows, rows, P("sp", None, "tp"), P("sp", None, "tp"), P("sp", "tp", None),
    )
    return jax.shard_map(
        per_device, mesh=mesh, in_specs=in_specs, out_specs=out_specs, check_vma=False
    )
```
